256 devices in a mesh: grp: 2 (over y), sp: 16 (over z), tp: 4 (over x), dp: 2 (over core).
Axes of the slice: x: 4, y: 2, z: 16, core: 2. Of those that a mesh axis runs over, the one named last changes fastest.
The devices are a block of a 4x16x16 slice.
Arguments:
- latent: bfloat16 [4, 6144, 2048], P(('grp', 'dp'), ('sp', 'tp')), parts along dimension 0, may hold values from -6 to 6
- cond: bfloat16 [4, 2048], P(('grp', 'dp')), parts along dimension 0, may hold values from -6 to 6
- context: bfloat16 [4, 256, 2048], P(('grp', 'dp'), 'sp'), parts along dimension 0, may hold values from -6 to 6
- cond_ctx: bfloat16 [2048], replicated, may hold values from -8 to 8
- w_shift: bfloat16 [2048, 2048], P('sp', 'tp'), may hold values from -0.125 to 0.125
- w_scale: bfloat16 [2048, 2048], P('sp', 'tp'), may hold values from -0.125 to 0.125
- w_gate: bfloat16 [2048, 2048], P('sp', 'tp'), may hold values from -0.125 to 0.125
- norm_gain: float32 [2048], replicated, may hold values from 0.1 to 1.9
- w_query: bfloat16 [2048, 1024], P(None, 'tp'), may hold values from -0.125 to 0.125
- w_key: bfloat16 [2048, 512], P(None, 'tp'), may hold values from -0.125 to 0.125
- w_value: bfloat16 [2048, 512], P(None, 'tp'), may hold values from -0.125 to 0.125
- query_gain: float32 [128], replicated, may hold values from 0.6 to 16
- key_gain: float32 [128], replicated, may hold values from 0.6 to 16
- ctx_lift: float32 [8], P('tp'), may hold values from -2 to 0.5
- out_gain: float32 [1024], replicated, may hold values from 0.1 to 1.9
- w_out: bfloat16 [1024, 2048], replicated, may hold values from -0.1875 to 0.1875
Outputs:
- result: bfloat16 [4, 6144, 2048], P(('grp', 'dp'), ('sp', 'tp')), parts along dimension 0
The draws below stay inside these ranges and needn't reach their ends.
There are 2 independent parts, one for each index of `grp`. The reference program is written for one: setup_inputs(seed, part) draws one part's arguments, and reference() takes and returns one part's arrays. A program takes and returns all parts, laid end to end along the dimension named above; an argument that names none is the same for every part. Nothing has to cross between parts.
All inputs are finite; a program needn't handle non-finite values.
Results may differ from the reference program's by a relative error of at most 0.023.
The reference program's roundings to bfloat16 on the way count: a program that leaves them out, or rounds other values in their place, can miss the bound.
Values may be sent and summed in bfloat16 or wider, within the bound.
A program may use at most 64 MiB of HBM per device.

```python
import math
import jax
import jax.numpy as jnp
from jax import lax

D = 2048
HEADS = 8
KV_HEADS = 4
HEAD_DIM = 128
GRID_WIDTH = 64
TOK_DEV = 384
CONTEXT = 256
BATCH = 2
TOKENS = 6144
N_SP = 16


def gain_common(key, role):
    logs = jax.random.uniform(jax.random.fold_in(key, role), (HEAD_DIM,), jnp.float32, jnp.log(0.6), jnp.log(2.2))
    base = jnp.exp(logs)
    return base


def draw_query_gain(key, part):
    return gain_common(key, 11)


def draw_key_gain(key, part):
    return gain_common(key, 12)


def level_of(own_key, extent, pieces, low, top_value):
    level, own = 1.0, jax.random.fold_in(own_key, 6)
    for dim, shards_of in pieces:
        heights = jnp.exp(jax.random.uniform(jax.random.fold_in(own, dim), (shards_of,), jnp.float32, low / len(pieces), top_value / len(pieces)))
        level = level * jnp.repeat(heights, extent[dim] // shards_of).reshape([-1 if axis == dim else 1 for axis in range(len(extent))])
    return level


def noise(stream_key, extent, scale, limit, cuts=(), kind=jnp.bfloat16):
    drawn = scale * jax.random.normal(stream_key, extent, jnp.float32)
    if cuts:
        drawn = drawn * level_of(stream_key, extent, cuts, -0.22, 0.18)
    return jnp.clip(drawn, -limit, limit).astype(kind)


def setup_inputs(seed: int = 0, part: int = 0) -> dict:
    keys = jax.random.split(jax.random.key(seed), 17)
    own_keys = jax.random.split(jax.random.fold_in(keys[16], part), 17)
    latent = noise(own_keys[0], (BATCH, TOKENS, D), 1.0, 6.0, ((0, 2), (1, 64)))
    cond = noise(own_keys[1], (BATCH, D), 1.0, 6.0, ((0, 2),))
    context = noise(own_keys[2], (BATCH, CONTEXT, D), 1.0, 6.0, ((0, 2), (1, 16)))
    cond_ctx = noise(keys[3], (D,), 2.0, 8.0)
    w_shift = noise(keys[4], (D, D), D ** -0.5, 0.125, ((0, 16), (1, 4)))
    w_scale = noise(keys[5], (D, D), D ** -0.5, 0.125, ((0, 16), (1, 4)))
    w_gate = noise(keys[6], (D, D), D ** -0.5, 0.125, ((0, 16), (1, 4)))
    norm_gain = jnp.clip(1.0 + 0.18 * jax.random.normal(keys[7], (D,), jnp.float32), 0.1, 1.9)
    w_query = noise(keys[8], (D, HEADS * HEAD_DIM), D ** -0.5, 0.125, ((1, 4),))
    w_key = noise(keys[9], (D, KV_HEADS * HEAD_DIM), D ** -0.5, 0.125, ((1, 4),))
    w_value = noise(keys[10], (D, KV_HEADS * HEAD_DIM), D ** -0.5, 0.125, ((1, 4),))
    query_gain = draw_query_gain(jax.random.fold_in(keys[16], 71), part)
    key_gain = draw_key_gain(jax.random.fold_in(keys[16], 71), part)
    ctx_lift = jnp.clip(-2.0 + 2.5 * jax.random.uniform(keys[13], (HEADS,), jnp.float32) ** level_of(keys[13], (HEADS,), ((0, 4),), -0.2, 0.2), -2.0, 0.5)
    out_gain = jnp.clip(1.0 + 0.18 * jax.random.normal(keys[14], (HEADS * HEAD_DIM,), jnp.float32), 0.1, 1.9)
    w_out = noise(keys[15], (HEADS * HEAD_DIM, D), (HEADS * HEAD_DIM) ** -0.5, 0.1875)
    return dict(latent=latent, cond=cond, context=context, cond_ctx=cond_ctx, w_shift=w_shift, w_scale=w_scale, w_gate=w_gate, norm_gain=norm_gain, w_query=w_query, w_key=w_key, w_value=w_value, query_gain=query_gain, key_gain=key_gain, ctx_lift=ctx_lift, out_gain=out_gain, w_out=w_out)


EPSILON = 1e-06

def rotate(vectors, positions):
    freqs = vectors.shape[-1] // 4
    grid_rows = (positions // GRID_WIDTH).astype(jnp.float32)
    grid_cols = (positions % GRID_WIDTH).astype(jnp.float32)
    inverse = 10000.0 ** (-jnp.arange(freqs, dtype=jnp.float32) / freqs)
    angles = jnp.stack([grid_rows[:, None] * inverse, grid_cols[:, None] * inverse], axis=1)
    cosine = jnp.cos(angles)[:, None]
    sine = jnp.sin(angles)[:, None]
    split = vectors.reshape(vectors.shape[:-1] + (2, 2, freqs))
    first = split[..., 0, :]
    second = split[..., 1, :]
    return jnp.stack([first * cosine - second * sine, second * cosine + first * sine], axis=-2).reshape(vectors.shape)

def head_norm(vectors, gain_vector):
    floats = vectors.astype(jnp.float32)
    return floats * lax.rsqrt(lax.optimization_barrier(jnp.mean(floats * floats, -1, keepdims=True)) + EPSILON) * gain_vector.astype(jnp.float32)

def modulated_norm(row_data, gain_vector, shift_row, scale_row):
    floats = row_data.astype(jnp.float32)
    normal = floats * lax.rsqrt(lax.optimization_barrier(jnp.mean(floats * floats, -1, keepdims=True)) + EPSILON)
    return (normal * gain_vector * (1.0 + scale_row) + shift_row).astype(jnp.bfloat16)

def reference(latent, cond, context, cond_ctx, w_shift, w_scale, w_gate, norm_gain, w_query, w_key, w_value, query_gain, key_gain, ctx_lift, out_gain, w_out):
    group = HEADS // KV_HEADS
    inputs = jax.nn.silu(jnp.concatenate([cond, cond_ctx[None]], 0).astype(jnp.float32)).astype(jnp.bfloat16)
    shift_all = jnp.dot(inputs, w_shift, preferred_element_type=jnp.float32)
    scale_all = jnp.dot(inputs, w_scale, preferred_element_type=jnp.float32)
    gate_all = jnp.dot(inputs, w_gate, preferred_element_type=jnp.float32)
    batch = latent.shape[0]
    positions = jnp.arange(TOKENS, dtype=jnp.int32)
    lift_table = (ctx_lift + math.log(TOKENS / CONTEXT)).reshape(KV_HEADS, group)
    factor = HEAD_DIM ** (-0.5)
    outputs = []
    for sample in range(batch):
        normed = modulated_norm(latent[sample], norm_gain, shift_all[sample], scale_all[sample])
        query_rows = jnp.dot(normed, w_query, preferred_element_type=jnp.float32).astype(jnp.bfloat16)
        key_rows = jnp.dot(normed, w_key, preferred_element_type=jnp.float32).astype(jnp.bfloat16)
        value_rows = jnp.dot(normed, w_value, preferred_element_type=jnp.float32).astype(jnp.bfloat16)
        query_rows = rotate(head_norm(query_rows.reshape(TOKENS, HEADS, HEAD_DIM), query_gain), positions).astype(jnp.bfloat16)
        query_rows = query_rows.reshape(TOKENS, KV_HEADS, group, HEAD_DIM)
        key_rows = rotate(head_norm(key_rows.reshape(TOKENS, KV_HEADS, HEAD_DIM), key_gain), positions).astype(jnp.bfloat16)
        value_rows = value_rows.reshape(TOKENS, KV_HEADS, HEAD_DIM)
        ctx_normed = modulated_norm(context[sample], norm_gain, shift_all[batch], scale_all[batch])
        ctx_key_rows = jnp.dot(ctx_normed, w_key, preferred_element_type=jnp.float32).astype(jnp.bfloat16)
        ctx_key_rows = head_norm(ctx_key_rows.reshape(CONTEXT, KV_HEADS, HEAD_DIM), key_gain).astype(jnp.bfloat16)
        ctx_value_rows = jnp.dot(ctx_normed, w_value, preferred_element_type=jnp.float32).astype(jnp.bfloat16)
        ctx_value_rows = ctx_value_rows.reshape(CONTEXT, KV_HEADS, HEAD_DIM)
        key_float = key_rows.astype(jnp.float32)
        value_float = value_rows.astype(jnp.float32)
        ctx_key_float = ctx_key_rows.astype(jnp.float32)
        ctx_value_float = ctx_value_rows.astype(jnp.float32)

        def attend(block_queries):
            query_float = block_queries.astype(jnp.float32)
            latent_scores = jnp.einsum('qkgd,nkd->kgqn', query_float, key_float) * factor
            ctx_scores = jnp.einsum('qkgd,nkd->kgqn', query_float, ctx_key_float) * factor + lift_table[:, :, None, None]
            highest = jnp.maximum(lax.optimization_barrier(jnp.max(latent_scores, -1)), lax.optimization_barrier(jnp.max(ctx_scores, -1)))[..., None]
            latent_exp = jnp.exp(latent_scores - highest)
            ctx_exp = jnp.exp(ctx_scores - highest)
            denominator = lax.optimization_barrier(jnp.sum(latent_exp, -1)) + lax.optimization_barrier(jnp.sum(ctx_exp, -1))
            latent_weights = latent_exp.astype(jnp.bfloat16).astype(jnp.float32)
            ctx_weights = ctx_exp.astype(jnp.bfloat16).astype(jnp.float32)
            summed = jnp.einsum('kgqn,nkd->qkgd', latent_weights, value_float) + jnp.einsum('kgqn,nkd->qkgd', ctx_weights, ctx_value_float)
            return (summed / jnp.transpose(denominator, (2, 0, 1))[..., None]).astype(jnp.bfloat16)
        blocks = query_rows.reshape(N_SP, TOK_DEV, KV_HEADS, group, HEAD_DIM)
        attended = lax.map(attend, blocks).reshape(TOKENS, HEADS * HEAD_DIM)
        att_normed = head_norm(attended, out_gain).astype(jnp.bfloat16)
        mixture = jnp.dot(att_normed, w_out, preferred_element_type=jnp.float32)
        outputs.append((latent[sample].astype(jnp.float32) + gate_all[sample] * mixture).astype(jnp.bfloat16))
    return jnp.stack(outputs)
```

```python
import functools
import math

import jax
import jax.numpy as jnp
from jax import lax
from jax.experimental import pallas as pl
from jax.experimental.pallas import tpu as pltpu
from jax.sharding import PartitionSpec as P

HEADS = 8
KV_HEADS = 4
HEAD_DIM = 128
GRID_WIDTH = 64
EPSILON = 1e-06
LOG2E = math.log2(math.e)
MESH = pl.DeviceIdType.MESH
F32 = jnp.float32
BF16 = jnp.bfloat16
RELATIVE = (0, 3, 1, 2)


def kernel(
    n_sp,
    latent,
    cond,
    context,
    cond_ctx,
    w_shift,
    w_scale,
    w_gate,
    norm_gain,
    w_query,
    w_key,
    w_value,
    query_gain,
    key_gain,
    ctx_lift,
    out_gain,
    w_out,
    result,
    lat,
    ctx_rows,
    wm,
    wq,
    wkv,
    wo,
    part,
    got_mod,
    got_gate,
    own_mod,
    own_gate,
    mod_all,
    gate_all,
    rows_mod,
    normed,
    cos_t,
    sin_t,
    kv_r,
    kv_l,
    q_s,
    m_s,
    l_s,
    acc_s,
    att_send,
    att_all,
    att_n,
    out_v,
    loc,
    x_send,
    x_recv,
    chain,
    p1_send,
    p1_recv,
    g1_send,
    g1_recv,
    p2_send,
    p2_recv,
    g2_send,
    g2_recv,
    r_send,
    r_recv,
    o_send,
    o_recv,
):
    z = lax.axis_index("sp")
    x = lax.axis_index("tp")
    n_tp = 4
    tok = lat.shape[1]
    half = tok // 2
    n_ctx = ctx_rows.shape[0]
    seq = n_tp * tok
    rows = n_ctx + seq
    width = lat.shape[2]
    mate = z + 1 - 2 * lax.rem(z, 2)
    parity = lax.rem(z, 2)

    def sp(d):
        return lax.rem(z + d + n_sp, n_sp)

    def tp(d):
        return lax.rem(x + d + n_tp, n_tp)

    def remote(src, dst, s, r, **where):
        return pltpu.make_async_remote_copy(
            src_ref=src,
            dst_ref=dst,
            send_sem=s,
            recv_sem=r,
            device_id=where,
            device_id_type=MESH,
        )

    loads = [
        pltpu.make_async_copy(latent.at[0], lat.at[0], loc.at[0]),
        pltpu.make_async_copy(w_shift, wm.at[0], loc.at[1]),
        pltpu.make_async_copy(w_scale, wm.at[1], loc.at[2]),
        pltpu.make_async_copy(w_gate, wm.at[2], loc.at[3]),
        pltpu.make_async_copy(context.at[0], ctx_rows, loc.at[4]),
        pltpu.make_async_copy(w_key, wkv.at[:, pl.ds(0, HEAD_DIM)], loc.at[5]),
        pltpu.make_async_copy(w_value, wkv.at[:, pl.ds(HEAD_DIM, HEAD_DIM)], loc.at[6]),
        pltpu.make_async_copy(w_query, wq, loc.at[7]),
        pltpu.make_async_copy(w_out, wo, loc.at[8]),
    ]
    for copy in loads:
        copy.start()

    barrier = pltpu.get_barrier_semaphore()
    near = [dict(sp=sp(1)), dict(sp=sp(-1))]
    near += [dict(tp=tp(d)) for d in range(1, n_tp)]
    near += [dict(tp=tp(d), sp=mate) for d in range(1, n_tp)]
    for where in near:
        pl.semaphore_signal(barrier, inc=1, device_id=where, device_id_type=MESH)
    pl.semaphore_wait(barrier, len(near))

    lo, hi = pl.ds(0, half), pl.ds(half, half)
    x_copies = [
        remote(lat.at[0, lo], lat.at[1, lo], x_send.at[0], x_recv.at[0], tp=tp(1)),
        remote(lat.at[0, hi], lat.at[2, hi], x_send.at[1], x_recv.at[1], tp=tp(-1)),
        remote(lat.at[0, hi], lat.at[1, hi], x_send.at[2], x_recv.at[2], tp=tp(1)),
        remote(lat.at[0, lo], lat.at[2, lo], x_send.at[3], x_recv.at[3], tp=tp(-1)),
        remote(lat.at[1, lo], lat.at[3, lo], x_send.at[4], x_recv.at[4], tp=tp(1)),
        remote(lat.at[2, hi], lat.at[3, hi], x_send.at[5], x_recv.at[5], tp=tp(-1)),
    ]
    loads[0].wait()
    for copy in x_copies[:4]:
        copy.start()

    in_rows = wm.shape[1]
    lanes = pl.ds(pl.multiple_of(z * in_rows, in_rows), in_rows)
    own_in = cond[:, lanes].astype(F32)
    ctx_in = cond_ctx[:, lanes].astype(F32)
    first_row = lax.broadcasted_iota(jnp.int32, (16, in_rows), 0) == 0
    both = jnp.where(
        first_row,
        jnp.broadcast_to(own_in, (16, in_rows)),
        jnp.broadcast_to(ctx_in, (16, in_rows)),
    )
    activated = jax.nn.silu(both).astype(BF16)
    for kind in range(3):
        loads[1 + kind].wait()
        product = jnp.dot(activated, wm[kind], preferred_element_type=F32)
        if kind < 2:
            for who in range(2):
                for block in range(2):
                    for side in range(2):
                        at = (2 * block + side) * 128
                        row = (2 * kind + who) * 2 + side
                        part[block, row : row + 1, :] = product[who : who + 1, at : at + 128]
        else:
            part[2, :, :] = jnp.zeros((8, 128), F32)
            for side in range(4):
                part[2, side : side + 1, :] = product[0:1, side * 128 : side * 128 + 128]

    reach, turn = 1, 0
    while 2 * reach <= n_sp // 2:
        for d in (reach, -reach):
            pl.semaphore_signal(
                chain.at[turn], inc=1, device_id=dict(sp=sp(d)), device_id_type=MESH
            )
        pl.semaphore_wait(chain.at[turn], 2)
        reach, turn = 2 * reach, turn + 1

    def p1(d):
        to = lax.rem(z + d, n_sp)
        return remote(
            part.at[lax.rem(to, 2)],
            got_mod.at[d - 1],
            p1_send.at[d - 1],
            p1_recv.at[d - 1],
            sp=to,
        )

    def g1(d):
        to = lax.rem(z + d, n_sp)
        return remote(
            part.at[2], got_gate.at[d - 1], g1_send.at[d - 1], g1_recv.at[d - 1], sp=to
        )

    def each(start, stop, f):
        def body(i, carry):
            f(i)
            return carry

        lax.fori_loop(start, stop, body, 0)

    each(1, n_sp, lambda d: p1(d).start())
    each(1, n_sp, lambda d: g1(d).start())

    cos_t[0:n_ctx, :] = jnp.ones((n_ctx, HEAD_DIM), F32)
    sin_t[0:n_ctx, :] = jnp.zeros((n_ctx, HEAD_DIM), F32)
    lane = lax.broadcasted_iota(jnp.int32, (tok, HEAD_DIM), 1)
    place = lax.broadcasted_iota(jnp.int32, (tok, HEAD_DIM), 0)
    quarter = HEAD_DIM // 4
    inverse = jnp.exp((lane & (quarter - 1)).astype(F32) * (-math.log(10000.0) / quarter))
    lower = (lane & (2 * quarter - 1)) < quarter
    for j in range(n_tp):
        token = z * seq + tp(RELATIVE[j]) * tok + place
        grid_row = token >> (GRID_WIDTH.bit_length() - 1)
        grid_col = token & (GRID_WIDTH - 1)
        angle = jnp.where(lane < 2 * quarter, grid_row, grid_col).astype(F32) * inverse
        at = n_ctx + j * tok
        cos_t[at : at + tok, :] = jnp.cos(angle)
        sine = jnp.sin(angle)
        sin_t[at : at + tok, :] = jnp.where(lower, -sine, sine)

    x_copies[0].wait_recv()
    x_copies[4].start()
    x_copies[1].wait_recv()
    x_copies[5].start()

    each(1, n_sp, lambda d: p1(d).wait_recv())

    def add_up(own, got):
        return lax.fori_loop(0, n_sp - 1, lambda i, total: total + got[i], own)

    own_mod[...] = add_up(part[parity], got_mod)
    mod_all[x, parity] = own_mod[...]
    spread = [(d, e) for e in range(2) for d in range(n_tp) if (d, e) != (0, 0)]
    p2 = []
    for i, (d, e) in enumerate(spread):
        where = {}
        if d:
            where["tp"] = tp(d)
        if e:
            where["sp"] = mate
        p2.append(
            remote(own_mod, mod_all.at[x, parity], p2_send.at[i], p2_recv.at[i], **where)
        )
    for copy in p2:
        copy.start()
    each(1, n_sp, lambda d: g1(d).wait_recv())
    own_gate[...] = add_up(part[2], got_gate)
    gate_all[x] = own_gate[...]
    g2 = [
        remote(own_gate, gate_all.at[x], g2_send.at[d - 1], g2_recv.at[d - 1], tp=tp(d))
        for d in range(1, n_tp)
    ]
    for copy in g2:
        copy.start()

    for copy in loads[4:8]:
        copy.wait()
    for copy in p2:
        copy.wait_recv()

    cols = width // n_tp
    for b in range(n_tp):
        for block in range(2):
            tile = mod_all[b, block]
            for side in range(2):
                at = b * cols + (2 * block + side) * 128
                gain = norm_gain[:, at : at + 128]
                for who in range(2):
                    r = who * 2 + side
                    rows_mod[who : who + 1, at : at + 128] = tile[r : r + 1, :]
                    rows_mod[2 + who : 3 + who, at : at + 128] = gain * (
                        1.0 + tile[4 + r : 5 + r, :]
                    )

    def norm_rows(read, base, count, who):
        shift = rows_mod[who : who + 1, :]
        scale = rows_mod[2 + who : 3 + who, :]

        def body(i, carry):
            floats = read(pl.ds(pl.multiple_of(i * 16, 16), 16)).astype(F32)
            inv = lax.rsqrt(jnp.mean(floats * floats, -1, keepdims=True) + EPSILON)
            normed[pl.ds(pl.multiple_of(base + i * 16, 16), 16), :] = (
                floats * inv * scale + shift
            ).astype(BF16)
            return carry

        lax.fori_loop(0, count // 16, body, 0)

    def head_norm(raw, gain):
        floats = raw.astype(BF16).astype(F32)
        return floats * lax.rsqrt(jnp.mean(floats * floats, -1, keepdims=True) + EPSILON) * gain

    def rotate(vectors, at, count):
        d = lax.broadcasted_iota(jnp.int32, (count, HEAD_DIM), 1)
        swapped = jnp.where(
            (d & (2 * quarter - 1)) < quarter,
            pltpu.roll(vectors, HEAD_DIM - quarter, 1),
            pltpu.roll(vectors, quarter, 1),
        )
        return vectors * cos_t[at : at + count, :] + swapped * sin_t[at : at + count, :]

    bounds = [(0, n_ctx + tok)] + [(n_ctx + j * tok, tok) for j in range(1, n_tp)]

    def ring(way, slot, j):
        at, count = bounds[j]
        buf = kv_r if way == 0 else kv_l
        piece = pl.ds(at, count)
        target = sp(1) if way == 0 else sp(-1)
        return remote(
            buf.at[slot - 1, :, piece],
            buf.at[slot, :, piece],
            r_send.at[way, slot - 1, j],
            r_recv.at[way, slot - 1, j],
            sp=target,
        )

    norm_rows(lambda i: ctx_rows[i, :], 0, n_ctx, 1)
    for j in range(n_tp):
        if j == 1:
            x_copies[2].wait_recv()
        if j == 2:
            x_copies[3].wait_recv()
        if j == 3:
            x_copies[4].wait_recv()
            x_copies[5].wait_recv()
        norm_rows(lambda i, j=j: lat[j, i, :], n_ctx + j * tok, tok, 0)
        at, count = bounds[j]
        made = jnp.dot(normed[at : at + count, :], wkv[...], preferred_element_type=F32)
        keys = rotate(head_norm(made[:, :HEAD_DIM], key_gain[...]), at, count).astype(BF16)
        values = made[:, HEAD_DIM:].astype(BF16)
        kv_r[0, 0, at : at + count, :] = keys
        kv_l[0, 0, at : at + count, :] = keys
        kv_r[0, 1, at : at + count, :] = values
        kv_l[0, 1, at : at + count, :] = values
        ring(0, 1, j).start()
        ring(1, 1, j).start()

    made = jnp.dot(normed[n_ctx:rows, :], wq[...], preferred_element_type=F32)
    for g in range(2):
        q_s[g] = rotate(
            head_norm(made[:, g * HEAD_DIM : (g + 1) * HEAD_DIM], query_gain[...]), n_ctx, seq
        ).astype(BF16)

    last = n_sp // 2
    factor = LOG2E * HEAD_DIM ** (-0.5)
    nt = (((1,), (1,)), ((), ()))

    def attend(g, keys, values, first=False, lift_from=None):
        scores = lax.dot_general(q_s[g], keys, nt, preferred_element_type=F32) * factor
        if lift_from is not None:
            lift = (ctx_lift[g] + math.log(seq / n_ctx)) * LOG2E
            at = lax.broadcasted_iota(jnp.int32, (1, keys.shape[0]), 1)
            scores = scores + jnp.where(at >= lift_from, lift, 0.0)
        top = jnp.max(scores, -1, keepdims=True)
        if not first:
            before = m_s[g]
            top = jnp.maximum(before, top)
        weights = jnp.exp2(scores - top)
        total = jnp.sum(weights, -1, keepdims=True)
        out = jnp.dot(weights.astype(BF16), values, preferred_element_type=F32)
        if not first:
            keep = jnp.exp2(before - top)
            total = total + l_s[g] * keep
            out = out + acc_s[g] * keep
        m_s[g] = top
        l_s[g] = total
        acc_s[g] = out

    def pull(s, j):
        for way in range(2):
            short = (j < 2) if way == 0 else (j >= 2)

            def wait(way=way):
                ring(way, s, j).wait_recv()

            def forward(way=way):
                ring(way, s + 1, j).start()

            if short:
                wait()
                pl.when(s < last)(forward)
            else:
                pl.when(s < last)(wait)
                pl.when(s < last - 1)(forward)

    body_rows = pl.ds(n_ctx, seq)
    for j in range(2):
        pull(1, j)
    attend(0, kv_r[0, 0, body_rows], kv_r[0, 1, body_rows], first=True)
    for j in range(2, 4):
        pull(1, j)
    attend(1, kv_r[0, 0, body_rows], kv_r[0, 1, body_rows], first=True)

    def step(s, carry):
        for g in range(2):
            for j in (2 * g, 2 * g + 1):
                pull(s, j)
            keys = jnp.concatenate([kv_r[s - 1, 0, body_rows], kv_l[s - 1, 0, body_rows]], 0)
            values = jnp.concatenate([kv_r[s - 1, 1, body_rows], kv_l[s - 1, 1, body_rows]], 0)
            attend(g, keys, values)
        return carry

    lax.fori_loop(2, last + 1, step, 0)

    def ending(kind):
        at, count = bounds[2]
        parts = [kv_r[last, kind, n_ctx:at], kv_l[last, kind, at:rows]]
        parts += [kv_r[s, kind, 0:n_ctx] for s in range(last + 1)]
        parts += [kv_l[s, kind, 0:n_ctx] for s in range(1, last)]
        return jnp.concatenate(parts, 0)

    end_keys = ending(0)
    end_values = ending(1)
    for g in range(2):
        attend(g, end_keys, end_values, lift_from=seq)
        att = (acc_s[g] / l_s[g]).astype(BF16)
        for j in range(n_tp):
            att_send[j, :, g * HEAD_DIM : (g + 1) * HEAD_DIM] = att[j * tok : (j + 1) * tok]

    exchange = [
        remote(
            att_send.at[j], att_all.at[x], o_send.at[j - 1], o_recv.at[j - 1], tp=tp(RELATIVE[j])
        )
        for j in range(1, n_tp)
    ]
    for copy in exchange:
        copy.start()
    att_all[x] = att_send[0]
    for copy in g2:
        copy.wait_recv()
    for b in range(n_tp):
        for side in range(4):
            at = b * cols + side * 128
            rows_mod[4:5, at : at + 128] = gate_all[b, side : side + 1, :]
    loads[8].wait()
    for copy in exchange:
        copy.wait_recv()

    channels = att_all.shape[2]
    pieces = [att_all[b].astype(F32) for b in range(n_tp)]
    square = sum(jnp.sum(p * p, -1, keepdims=True) for p in pieces)
    inv = lax.rsqrt(square * (1.0 / (n_tp * channels)) + EPSILON)
    for b in range(n_tp):
        gain = out_gain[:, b * channels : (b + 1) * channels]
        att_n[:, b * channels : (b + 1) * channels] = (pieces[b] * inv * gain).astype(BF16)
    strip = 512
    stores = []
    for i in range(width // strip):
        at = pl.ds(i * strip, strip)
        mix = jnp.dot(att_n[...], wo[:, at], preferred_element_type=F32)
        out_v[:, at] = (lat[0, :, at].astype(F32) + rows_mod[4:5, at] * mix).astype(BF16)
        store = pltpu.make_async_copy(out_v.at[:, at], result.at[0, :, at], loc.at[9 + i])
        store.start()
        stores.append(store)

    for copy in x_copies + p2 + g2 + exchange:
        copy.wait_send()
    each(1, n_sp, lambda d: p1(d).wait_send())
    each(1, n_sp, lambda d: g1(d).wait_send())

    def drain(s, carry):
        for j in range(4):
            for way in range(2):
                short = (j < 2) if way == 0 else (j >= 2)

                def wait(way=way, j=j):
                    ring(way, s, j).wait_send()

                if short:
                    wait()
                else:
                    pl.when(s < last)(wait)
        return carry

    lax.fori_loop(1, last + 1, drain, 0)
    for store in stores:
        store.wait()


def on_device(mesh, *args):
    (
        latent,
        cond,
        context,
        cond_ctx,
        w_shift,
        w_scale,
        w_gate,
        norm_gain,
        w_query,
        w_key,
        w_value,
        query_gain,
        key_gain,
        ctx_lift,
        out_gain,
        w_out,
    ) = args
    n_sp, n_tp = mesh.shape["sp"], mesh.shape["tp"]
    assert n_tp == 4 and KV_HEADS == n_tp and n_sp % 4 == 0
    tok, width = latent.shape[1:]
    n_ctx = context.shape[1]
    rows = n_ctx + n_tp * tok
    seq = n_tp * tok
    slots = n_sp // 2 + 1
    any_ = pl.BlockSpec(memory_space=pl.ANY)
    vmem = pl.BlockSpec(memory_space=pltpu.VMEM)
    smem = pl.BlockSpec(memory_space=pltpu.SMEM)
    dma = pltpu.SemaphoreType.DMA
    scratch = [
        pltpu.VMEM((n_tp, tok, width), BF16),
        pltpu.VMEM((n_ctx, width), BF16),
        pltpu.VMEM((3,) + w_shift.shape, BF16),
        pltpu.VMEM(w_query.shape, BF16),
        pltpu.VMEM((width, 2 * HEAD_DIM), BF16),
        pltpu.VMEM(w_out.shape, BF16),
        pltpu.VMEM((3, 8, 128), F32),
        pltpu.VMEM((n_sp - 1, 8, 128), F32),
        pltpu.VMEM((n_sp - 1, 8, 128), F32),
        pltpu.VMEM((8, 128), F32),
        pltpu.VMEM((8, 128), F32),
        pltpu.VMEM((n_tp, 2, 8, 128), F32),
        pltpu.VMEM((n_tp, 8, 128), F32),
        pltpu.VMEM((8, width), F32),
        pltpu.VMEM((rows, width), BF16),
        pltpu.VMEM((rows, HEAD_DIM), F32),
        pltpu.VMEM((rows, HEAD_DIM), F32),
        pltpu.VMEM((slots, 2, rows, HEAD_DIM), BF16),
        pltpu.VMEM((slots, 2, rows, HEAD_DIM), BF16),
        pltpu.VMEM((2, seq, HEAD_DIM), BF16),
        pltpu.VMEM((2, seq, 1), F32),
        pltpu.VMEM((2, seq, 1), F32),
        pltpu.VMEM((2, seq, HEAD_DIM), F32),
        pltpu.VMEM((n_tp, tok, 2 * HEAD_DIM), BF16),
        pltpu.VMEM((n_tp, tok, 2 * HEAD_DIM), BF16),
        pltpu.VMEM((tok, HEADS * HEAD_DIM), BF16),
        pltpu.VMEM((tok, width), BF16),
        dma((13,)),
        dma((6,)),
        dma((6,)),
        pltpu.SemaphoreType.REGULAR((3,)),
        dma((n_sp - 1,)),
        dma((n_sp - 1,)),
        dma((n_sp - 1,)),
        dma((n_sp - 1,)),
        dma((7,)),
        dma((7,)),
        dma((3,)),
        dma((3,)),
        dma((2, slots - 1, 4)),
        dma((2, slots - 1, 4)),
        dma((3,)),
        dma((3,)),
    ]
    specs = [any_, vmem, any_, vmem, any_, any_, any_, vmem]
    specs += [any_, any_, any_, vmem, vmem, smem, vmem, any_]
    row = lambda a: a.reshape(1, -1)
    return pl.pallas_call(
        functools.partial(kernel, n_sp),
        out_shape=jax.ShapeDtypeStruct(latent.shape, BF16),
        in_specs=specs,
        out_specs=any_,
        scratch_shapes=scratch,
        compiler_params=pltpu.CompilerParams(
            collective_id=0, has_side_effects=True, vmem_limit_bytes=56 << 20
        ),
    )(
        latent,
        cond,
        context,
        row(cond_ctx),
        w_shift,
        w_scale,
        w_gate,
        row(norm_gain),
        w_query,
        w_key,
        w_value,
        row(query_gain),
        row(key_gain),
        ctx_lift,
        row(out_gain),
        w_out,
    )


def solution(mesh):
    in_specs = (
        P(("grp", "dp"), ("sp", "tp"), None),
        P(("grp", "dp"), None),
        P(("grp", "dp"), "sp", None),
        P(),
        P("sp", "tp"),
        P("sp", "tp"),
        P("sp", "tp"),
        P(),
        P(None, "tp"),
        P(None, "tp"),
        P(None, "tp"),
        P(),
        P(),
        P("tp"),
        P(),
        P(),
    )
    out_specs = P(("grp", "dp"), ("sp", "tp"), None)
    return jax.shard_map(
        functools.partial(on_device, mesh),
        mesh=mesh,
        in_specs=in_specs,
        out_specs=out_specs,
        check_vma=False,
    )
```

```python
import functools
import math

import jax
import jax.numpy as jnp
from jax import lax
from jax.experimental import pallas as pl
from jax.experimental.pallas import tpu as pltpu
from jax.sharding import PartitionSpec as P

HEADS = 8
KV_HEADS = 4
HEAD_DIM = 128
GRID_WIDTH = 64
EPSILON = 1e-06
LOG2E = math.log2(math.e)
MESH = pl.DeviceIdType.MESH
F32 = jnp.float32
BF16 = jnp.bfloat16
RELATIVE = (0, 3, 1, 2)


def kernel(
    n_sp,
    latent,
    cond_h,
    context,
    cond_ctx_h,
    w_shift,
    w_scale,
    w_gate,
    norm_gain_h,
    w_query,
    w_key,
    w_value,
    query_gain_h,
    key_gain_h,
    ctx_lift,
    out_gain_h,
    w_out,
    result,
    cond,
    cond_ctx,
    norm_gain,
    query_gain,
    key_gain,
    out_gain,
    lat,
    ctx_rows,
    wm,
    wq,
    wkv,
    wo,
    part,
    got_mod,
    own_mod,
    mod_all,
    rows_mod,
    unit,
    normed,
    cos_t,
    sin_t,
    kv_r,
    kv_l,
    q_s,
    m_s,
    l_s,
    acc_s,
    att_send,
    att_all,
    att_n,
    out_v,
    loc,
    x_send,
    x_recv,
    p1_send,
    p1_recv,
    p2_send,
    p2_recv,
    r_send,
    r_recv,
    o_send,
    o_recv,
):
    z = lax.axis_index("sp")
    x = lax.axis_index("tp")
    n_tp = 4
    tok = lat.shape[1]
    half = tok // 2
    n_ctx = ctx_rows.shape[0]
    seq = n_tp * tok
    rows = n_ctx + seq
    width = lat.shape[2]
    mate = z + 1 - 2 * lax.rem(z, 2)
    parity = lax.rem(z, 2)

    def sp(d):
        return lax.rem(z + d + n_sp, n_sp)

    def tp(d):
        return lax.rem(x + d + n_tp, n_tp)

    def remote(src, dst, s, r, **where):
        return pltpu.make_async_remote_copy(
            src_ref=src,
            dst_ref=dst,
            send_sem=s,
            recv_sem=r,
            device_id=where,
            device_id_type=MESH,
        )

    def each(start, stop, f):
        def body(i, carry):
            f(i)
            return carry

        lax.fori_loop(start, stop, body, 0)

    barrier = pltpu.get_barrier_semaphore()

    def greet(**where):
        pl.semaphore_signal(barrier, inc=1, device_id=where, device_id_type=MESH)

    for d in range(1, n_tp):
        greet(tp=tp(d))
        greet(tp=tp(d), sp=mate)
    each(1, n_sp, lambda d: greet(sp=lax.rem(z + d, n_sp)))

    def load(src, dst, i):
        copy = pltpu.make_async_copy(src, dst, loc.at[i])
        copy.start()
        return copy

    load_cond = load(cond_h, cond, 0)
    load_cond_ctx = load(cond_ctx_h, cond_ctx, 1)
    for kind, matrix in enumerate((w_shift, w_scale, w_gate)):
        load(matrix, wm.at[kind], 2)
    load_lat = load(latent.at[0], lat.at[0], 3)
    load_ctx = load(context.at[0], ctx_rows, 4)
    load(w_key, wkv.at[:, pl.ds(0, HEAD_DIM)], 5)
    load(w_value, wkv.at[:, pl.ds(HEAD_DIM, HEAD_DIM)], 5)
    load_gain = load(norm_gain_h, norm_gain, 6)
    load_key_gain = load(key_gain_h, key_gain, 7)
    load_wq = load(w_query, wq, 8)
    load_query_gain = load(query_gain_h, query_gain, 9)
    load_wo = load(w_out, wo, 10)
    load_out_gain = load(out_gain_h, out_gain, 11)

    def arrived(whole, i):
        pltpu.make_async_copy(whole, whole, loc.at[i]).wait()

    in_rows = wm.shape[1]
    load_cond.wait()
    load_cond_ctx.wait()
    lanes = pl.ds(pl.multiple_of(z * in_rows, in_rows), in_rows)
    own_in = cond[:, lanes].astype(F32)
    every = cond_ctx[...].astype(F32)
    line = lax.broadcasted_iota(jnp.int32, every.shape, 0)
    ctx_in = jnp.sum(jnp.where(line == z, every, 0.0), 0, keepdims=True)
    first_row = lax.broadcasted_iota(jnp.int32, (16, in_rows), 0) == 0
    both = jnp.where(
        first_row,
        jnp.broadcast_to(own_in, (16, in_rows)),
        jnp.broadcast_to(ctx_in, (16, in_rows)),
    )
    activated = jax.nn.silu(both).astype(BF16)
    arrived(wm, 2)
    for kind in range(3):
        product = jnp.dot(activated, wm[kind], preferred_element_type=F32)
        for who in range(2 if kind < 2 else 1):
            for block in range(2):
                for side in range(2):
                    at = (2 * block + side) * 128
                    row = (2 * kind + who) * 2 + side
                    part[block, row : row + 1, :] = product[who : who + 1, at : at + 128]

    load_lat.wait()
    pl.semaphore_wait(barrier, n_sp - 1 + 2 * (n_tp - 1))

    used = pl.ds(0, 10)

    def p1(d):
        to = lax.rem(z + d, n_sp)
        return remote(
            part.at[lax.rem(to, 2), used],
            got_mod.at[d - 1, used],
            p1_send.at[0],
            p1_recv.at[0],
            sp=to,
        )

    each(1, n_sp, lambda d: p1(d).start())

    lo, hi = pl.ds(0, half), pl.ds(half, half)
    x_copies = [
        remote(lat.at[0, lo], lat.at[1, lo], x_send.at[0], x_recv.at[0], tp=tp(1)),
        remote(lat.at[0, hi], lat.at[2, hi], x_send.at[0], x_recv.at[1], tp=tp(-1)),
        remote(lat.at[0, hi], lat.at[1, hi], x_send.at[0], x_recv.at[2], tp=tp(1)),
        remote(lat.at[0, lo], lat.at[2, lo], x_send.at[0], x_recv.at[3], tp=tp(-1)),
        remote(lat.at[1, lo], lat.at[3, lo], x_send.at[0], x_recv.at[4], tp=tp(1)),
        remote(lat.at[2, hi], lat.at[3, hi], x_send.at[0], x_recv.at[4], tp=tp(-1)),
    ]
    for copy in x_copies[:4]:
        copy.start()

    cos_t[0:n_ctx, :] = jnp.ones((n_ctx, HEAD_DIM), F32)
    sin_t[0:n_ctx, :] = jnp.zeros((n_ctx, HEAD_DIM), F32)
    lane = lax.broadcasted_iota(jnp.int32, (tok, HEAD_DIM), 1)
    place = lax.broadcasted_iota(jnp.int32, (tok, HEAD_DIM), 0)
    quarter = HEAD_DIM // 4
    inverse = jnp.exp((lane & (quarter - 1)).astype(F32) * (-math.log(10000.0) / quarter))
    lower = (lane & (2 * quarter - 1)) < quarter
    for j in range(n_tp):
        token = z * seq + tp(RELATIVE[j]) * tok + place
        grid_row = token >> (GRID_WIDTH.bit_length() - 1)
        grid_col = token & (GRID_WIDTH - 1)
        angle = jnp.where(lane < 2 * quarter, grid_row, grid_col).astype(F32) * inverse
        at = n_ctx + j * tok
        cos_t[at : at + tok, :] = jnp.cos(angle)
        sine = jnp.sin(angle)
        sin_t[at : at + tok, :] = jnp.where(lower, -sine, sine)

    def prepare(read, base, count):
        def body(i, carry):
            floats = read(pl.ds(pl.multiple_of(i * 16, 16), 16)).astype(F32)
            inv = lax.rsqrt(jnp.mean(floats * floats, -1, keepdims=True) + EPSILON)
            unit[pl.ds(pl.multiple_of(base + i * 16, 16), 16), :] = floats * inv
            return carry

        lax.fori_loop(0, count // 16, body, 0)

    load_ctx.wait()
    prepare(lambda i: ctx_rows[i, :], 0, n_ctx)
    prepare(lambda i: lat[0, i, :], n_ctx, tok)
    arrived(wkv, 5)
    load_gain.wait()
    load_key_gain.wait()

    every_got = got_mod.at[:, used]
    remote(every_got, every_got, p1_send.at[0], p1_recv.at[0], sp=mate).wait_recv()
    own_mod[...] = lax.fori_loop(
        0, n_sp - 1, lambda i, total: total + got_mod[i, 0:10, :], part[parity, 0:10, :]
    )
    mod_all[x, parity, 0:10, :] = own_mod[...]
    spread = [(d, e) for e in (1, 0) for d in (2, 1, 3, 0) if (d, e) != (0, 0)]
    p2 = []
    for i, (d, e) in enumerate(spread):
        where = {}
        if d:
            where["tp"] = tp(d)
        if e:
            where["sp"] = mate
        p2.append(
            remote(own_mod, mod_all.at[x, parity, used], p2_send.at[0], p2_recv.at[i], **where)
        )
    for copy in p2:
        copy.start()

    x_copies[0].wait_recv()
    x_copies[4].start()
    x_copies[1].wait_recv()
    x_copies[5].start()
    x_copies[2].wait_recv()
    prepare(lambda i: lat[1, i, :], n_ctx + tok, tok)
    x_copies[3].wait_recv()
    prepare(lambda i: lat[2, i, :], n_ctx + 2 * tok, tok)
    for copy in p2:
        copy.wait_recv()

    cols = width // n_tp
    for b in range(n_tp):
        for block in range(2):
            tile = mod_all[b, block, 0:10, :]
            for side in range(2):
                at = b * cols + (2 * block + side) * 128
                gain = norm_gain[:, at : at + 128]
                for who in range(2):
                    r = who * 2 + side
                    rows_mod[who : who + 1, at : at + 128] = tile[r : r + 1, :]
                    rows_mod[2 + who : 3 + who, at : at + 128] = gain * (
                        1.0 + tile[4 + r : 5 + r, :]
                    )
                rows_mod[4:5, at : at + 128] = tile[8 + side : 9 + side, :]

    def norm_rows(base, count, who):
        shift = rows_mod[who : who + 1, :]
        scale = rows_mod[2 + who : 3 + who, :]

        def body(i, carry):
            at = pl.ds(pl.multiple_of(base + i * 16, 16), 16)
            normed[at, :] = (unit[at, :] * scale + shift).astype(BF16)
            return carry

        lax.fori_loop(0, count // 16, body, 0)

    def head_norm(raw, gain):
        floats = raw.astype(BF16).astype(F32)
        return floats * lax.rsqrt(jnp.mean(floats * floats, -1, keepdims=True) + EPSILON) * gain

    def rotate(vectors, at, count):
        d = lax.broadcasted_iota(jnp.int32, (count, HEAD_DIM), 1)
        swapped = jnp.where(
            (d & (2 * quarter - 1)) < quarter,
            pltpu.roll(vectors, HEAD_DIM - quarter, 1),
            pltpu.roll(vectors, quarter, 1),
        )
        return vectors * cos_t[at : at + count, :] + swapped * sin_t[at : at + count, :]

    bounds = [(0, n_ctx + tok)] + [(n_ctx + j * tok, tok) for j in range(1, n_tp)]

    def ring(way, slot, j, final=False):
        at, count = bounds[j]
        buf = kv_r if way == 0 else kv_l
        piece = pl.ds(at, count)
        target = sp(1) if way == 0 else sp(-1)
        return remote(
            buf.at[slot - 1, :, piece],
            buf.at[slot, :, piece],
            r_send.at[way + 2 if final else way],
            r_recv.at[way, slot - 1, j],
            sp=target,
        )

    norm_rows(0, n_ctx, 1)
    for j in range(n_tp):
        at, count = bounds[j]
        if j == 3:
            remote(lat.at[3], lat.at[3], x_send.at[0], x_recv.at[4], tp=tp(1)).wait_recv()
            prepare(lambda i: lat[3, i, :], n_ctx + 3 * tok, tok)
        norm_rows(n_ctx + j * tok, tok, 0)
        made = jnp.dot(normed[at : at + count, :], wkv[...], preferred_element_type=F32)
        keys = rotate(head_norm(made[:, :HEAD_DIM], key_gain[...]), at, count).astype(BF16)
        values = made[:, HEAD_DIM:].astype(BF16)
        kv_r[0, 0, at : at + count, :] = keys
        kv_l[0, 0, at : at + count, :] = keys
        kv_r[0, 1, at : at + count, :] = values
        kv_l[0, 1, at : at + count, :] = values
        ring(0, 1, j).start()
        ring(1, 1, j).start()

    last = n_sp // 2
    factor = LOG2E * HEAD_DIM ** (-0.5)
    nt = (((1,), (1,)), ((), ()))

    def attend(g, keys, values, first=False, lift_from=None):
        scores = lax.dot_general(q_s[g], keys, nt, preferred_element_type=F32) * factor
        if lift_from is not None:
            lift = (ctx_lift[g] + math.log(seq / n_ctx)) * LOG2E
            at = lax.broadcasted_iota(jnp.int32, (1, keys.shape[0]), 1)
            scores = scores + jnp.where(at >= lift_from, lift, 0.0)
        top = jnp.max(scores, -1, keepdims=True)
        if not first:
            before = m_s[g]
            top = jnp.maximum(before, top)
        weights = jnp.exp2(scores - top)
        total = jnp.sum(weights, -1, keepdims=True)
        out = jnp.dot(weights.astype(BF16), values, preferred_element_type=F32)
        if not first:
            keep = jnp.exp2(before - top)
            total = total + l_s[g] * keep
            out = out + acc_s[g] * keep
        m_s[g] = top
        l_s[g] = total
        acc_s[g] = out

    def pull(s, j):
        for way in range(2):
            short = (j < 2) if way == 0 else (j >= 2)

            def wait(way=way):
                ring(way, s, j).wait_recv()

            def forward(final, way=way):
                ring(way, s + 1, j, final).start()

            if isinstance(s, int):
                if s < last or short:
                    wait()
                if s + 1 < last:
                    forward(False)
                elif s + 1 == last and short:
                    forward(True)
                continue
            wait()
            pl.when(s + 1 < last)(functools.partial(forward, False))
            if short:
                pl.when(s + 1 == last)(functools.partial(forward, True))

    body_rows = pl.ds(n_ctx, seq)
    pull(1, 0)
    load_wq.wait()
    load_query_gain.wait()
    made = jnp.dot(normed[n_ctx:rows, :], wq[...], preferred_element_type=F32)
    for g in range(2):
        q_s[g] = rotate(
            head_norm(made[:, g * HEAD_DIM : (g + 1) * HEAD_DIM], query_gain[...]), n_ctx, seq
        ).astype(BF16)
    pull(1, 1)
    attend(0, kv_r[0, 0, body_rows], kv_r[0, 1, body_rows], first=True)
    pull(1, 2)
    pull(1, 3)
    attend(1, kv_r[0, 0, body_rows], kv_r[0, 1, body_rows], first=True)

    def pair(slot, kind):
        return jnp.concatenate([kv_r[slot, kind, body_rows], kv_l[slot, kind, body_rows]], 0)

    def step(s, carry):
        for g in range(2):
            for j in (2 * g, 2 * g + 1):
                pull(s, j)
            attend(g, pair(s - 1, 0), pair(s - 1, 1))
        return carry

    lax.fori_loop(2, last, step, 0)
    for g in range(2):
        attend(g, pair(last - 1, 0), pair(last - 1, 1))

    def chunk(way, kind, j):
        at = n_ctx + j * tok
        return (kv_r if way == 0 else kv_l)[last, kind, at : at + tok]

    def ending(kind):
        parts = [chunk(0, kind, 0), chunk(1, kind, 2)]
        parts += [kv_r[s, kind, 0:n_ctx] for s in range(last + 1)]
        parts += [kv_l[s, kind, 0:n_ctx] for s in range(1, last)]
        return jnp.concatenate(parts, 0)

    pull(last, 0)
    pull(last, 2)
    for g in range(2):
        attend(g, ending(0), ending(1), lift_from=2 * tok)
    pull(last, 1)
    pull(last, 3)

    def exchange(g, j):
        part_of = pl.ds(g * HEAD_DIM, HEAD_DIM)
        return remote(
            att_send.at[j, :, part_of],
            att_all.at[x, :, part_of],
            o_send.at[0],
            o_recv.at[j - 1],
            tp=tp(RELATIVE[j]),
        )

    for g in range(2):
        attend(
            g,
            jnp.concatenate([chunk(0, 0, 1), chunk(1, 0, 3)], 0),
            jnp.concatenate([chunk(0, 1, 1), chunk(1, 1, 3)], 0),
        )
        att = (acc_s[g] / l_s[g]).astype(BF16)
        for j in range(n_tp):
            att_send[j, :, g * HEAD_DIM : (g + 1) * HEAD_DIM] = att[j * tok : (j + 1) * tok]
        for j in (3, 1, 2):
            exchange(g, j).start()
    att_all[x] = att_send[0]
    load_wo.wait()
    load_out_gain.wait()
    for j in range(1, n_tp):
        whole = att_all.at[tp(-RELATIVE[j])]
        remote(whole, whole, o_send.at[0], o_recv.at[j - 1], tp=tp(1)).wait_recv()

    channels = att_all.shape[2]
    pieces = [att_all[b].astype(F32) for b in range(n_tp)]
    square = sum(jnp.sum(p * p, -1, keepdims=True) for p in pieces)
    inv = lax.rsqrt(square * (1.0 / (n_tp * channels)) + EPSILON)
    for b in range(n_tp):
        gain = out_gain[:, b * channels : (b + 1) * channels]
        att_n[:, b * channels : (b + 1) * channels] = (pieces[b] * inv * gain).astype(BF16)
    strip = 512
    for i in range(width // strip):
        at = pl.ds(i * strip, strip)
        mix = jnp.dot(att_n[...], wo[:, at], preferred_element_type=F32)
        out_v[:, at] = (lat[0, :, at].astype(F32) + rows_mod[4:5, at] * mix).astype(BF16)
        pltpu.make_async_copy(out_v.at[:, at], result.at[0, :, at], loc.at[12]).start()

    def sent(whole, sem):
        remote(whole, whole, sem, p1_recv.at[0], sp=mate).wait_send()

    sent(lat.at[0:3], x_send.at[0])
    sent(every_got, p1_send.at[0])
    sent(got_mod.at[0 : len(p2), used], p2_send.at[0])
    sent(kv_r.at[0 : last - 1], r_send.at[0])
    sent(kv_l.at[0 : last - 1], r_send.at[1])
    at, _ = bounds[2]
    sent(kv_r.at[last - 1, :, 0:at], r_send.at[2])
    sent(kv_l.at[last - 1, :, at:rows], r_send.at[3])
    sent(att_send.at[1:n_tp], o_send.at[0])
    pltpu.make_async_copy(out_v, result.at[0], loc.at[12]).wait()


def on_device(mesh, *args):
    (
        latent,
        cond,
        context,
        cond_ctx,
        w_shift,
        w_scale,
        w_gate,
        norm_gain,
        w_query,
        w_key,
        w_value,
        query_gain,
        key_gain,
        ctx_lift,
        out_gain,
        w_out,
    ) = args
    n_sp, n_tp = mesh.shape["sp"], mesh.shape["tp"]
    assert n_tp == 4 and KV_HEADS == n_tp and n_sp % 4 == 0
    assert w_shift.shape == (128, 512)
    tok, width = latent.shape[1:]
    n_ctx = context.shape[1]
    rows = n_ctx + n_tp * tok
    seq = n_tp * tok
    slots = n_sp // 2 + 1
    any_ = pl.BlockSpec(memory_space=pl.ANY)
    smem = pl.BlockSpec(memory_space=pltpu.SMEM)
    dma = pltpu.SemaphoreType.DMA
    scratch = [
        pltpu.VMEM((1, width), BF16),
        pltpu.VMEM((width // 128, 128), BF16),
        pltpu.VMEM((1, width), F32),
        pltpu.VMEM((1, HEAD_DIM), F32),
        pltpu.VMEM((1, HEAD_DIM), F32),
        pltpu.VMEM((1, HEADS * HEAD_DIM), F32),
        pltpu.VMEM((n_tp, tok, width), BF16),
        pltpu.VMEM((n_ctx, width), BF16),
        pltpu.VMEM((3,) + w_shift.shape, BF16),
        pltpu.VMEM(w_query.shape, BF16),
        pltpu.VMEM((width, 2 * HEAD_DIM), BF16),
        pltpu.VMEM(w_out.shape, BF16),
        pltpu.VMEM((2, 16, 128), F32),
        pltpu.VMEM((n_sp - 1, 16, 128), F32),
        pltpu.VMEM((10, 128), F32),
        pltpu.VMEM((n_tp, 2, 16, 128), F32),
        pltpu.VMEM((8, width), F32),
        pltpu.VMEM((rows, width), F32),
        pltpu.VMEM((rows, width), BF16),
        pltpu.VMEM((rows, HEAD_DIM), F32),
        pltpu.VMEM((rows, HEAD_DIM), F32),
        pltpu.VMEM((slots, 2, rows, HEAD_DIM), BF16),
        pltpu.VMEM((slots, 2, rows, HEAD_DIM), BF16),
        pltpu.VMEM((2, seq, HEAD_DIM), BF16),
        pltpu.VMEM((2, seq, 1), F32),
        pltpu.VMEM((2, seq, 1), F32),
        pltpu.VMEM((2, seq, HEAD_DIM), F32),
        pltpu.VMEM((n_tp, tok, 2 * HEAD_DIM), BF16),
        pltpu.VMEM((n_tp, tok, 2 * HEAD_DIM), BF16),
        pltpu.VMEM((tok, HEADS * HEAD_DIM), BF16),
        pltpu.VMEM((tok, width), BF16),
        dma((13,)),
        dma((1,)),
        dma((5,)),
        dma((1,)),
        dma((1,)),
        dma((1,)),
        dma((7,)),
        dma((4,)),
        dma((2, slots - 1, 4)),
        dma((1,)),
        dma((3,)),
    ]
    specs = [any_] * 13 + [smem, any_, any_]
    row = lambda a: a.reshape(1, -1)
    return pl.pallas_call(
        functools.partial(kernel, n_sp),
        out_shape=jax.ShapeDtypeStruct(latent.shape, BF16),
        in_specs=specs,
        out_specs=any_,
        scratch_shapes=scratch,
        compiler_params=pltpu.CompilerParams(
            collective_id=0, has_side_effects=True, vmem_limit_bytes=56 << 20
        ),
    )(
        latent,
        cond,
        context,
        cond_ctx.reshape(-1, 128),
        w_shift,
        w_scale,
        w_gate,
        row(norm_gain),
        w_query,
        w_key,
        w_value,
        row(query_gain),
        row(key_gain),
        ctx_lift,
        row(out_gain),
        w_out,
    )


def solution(mesh):
    in_specs = (
        P(("grp", "dp"), ("sp", "tp"), None),
        P(("grp", "dp"), None),
        P(("grp", "dp"), "sp", None),
        P(),
        P("sp", "tp"),
        P("sp", "tp"),
        P("sp", "tp"),
        P(),
        P(None, "tp"),
        P(None, "tp"),
        P(None, "tp"),
        P(),
        P(),
        P("tp"),
        P(),
        P(),
    )
    out_specs = P(("grp", "dp"), ("sp", "tp"), None)
    return jax.shard_map(
        functools.partial(on_device, mesh),
        mesh=mesh,
        in_specs=in_specs,
        out_specs=out_specs,
        check_vma=False,
    )
```

```python
import functools
import math

import jax
import jax.numpy as jnp
from jax import lax
from jax.experimental import pallas as pl
from jax.experimental.pallas import tpu as pltpu
from jax.sharding import PartitionSpec as P

HEADS = 8
KV_HEADS = 4
HEAD_DIM = 128
GRID_WIDTH = 64
EPSILON = 1e-06
LOG2E = math.log2(math.e)
MESH = pl.DeviceIdType.MESH
F32 = jnp.float32
BF16 = jnp.bfloat16
RELATIVE = (0, 3, 1, 2)


def kernel(
    n_sp,
    latent,
    cond_h,
    context,
    cond_ctx_h,
    w_shift,
    w_scale,
    w_gate,
    norm_gain_h,
    w_query,
    w_key,
    w_value,
    query_gain_h,
    key_gain_h,
    ctx_lift,
    out_gain_h,
    w_out,
    result,
    cond,
    cond_ctx,
    norm_gain,
    query_gain,
    key_gain,
    out_gain,
    lat,
    ctx_rows,
    wm,
    wq,
    wkv,
    wo,
    part,
    got_mod,
    window,
    got_half,
    own_mod,
    mod_all,
    rows_mod,
    unit,
    normed,
    cos_t,
    sin_t,
    kv_r,
    kv_l,
    q_s,
    m_s,
    l_s,
    acc_s,
    att_send,
    att_all,
    att_n,
    loc,
    x_send,
    x_recv,
    p1_send,
    p1_recv,
    h_send,
    h_recv,
    p2_send,
    p2_recv,
    r_send,
    r_recv,
    o_send,
    o_recv,
):
    z = lax.axis_index("sp")
    x = lax.axis_index("tp")
    n_tp = 4
    tok = lat.shape[1]
    half = tok // 2
    n_ctx = ctx_rows.shape[0]
    seq = n_tp * tok
    rows = n_ctx + seq
    width = lat.shape[2]
    reach = n_sp // 4
    mate = z + 1 - 2 * lax.rem(z, 2)
    parity = lax.rem(z, 2)

    def sp(d):
        return lax.rem(z + d + n_sp, n_sp)

    def tp(d):
        return lax.rem(x + d + n_tp, n_tp)

    def remote(src, dst, s, r, **where):
        return pltpu.make_async_remote_copy(
            src_ref=src,
            dst_ref=dst,
            send_sem=s,
            recv_sem=r,
            device_id=where,
            device_id_type=MESH,
        )

    def each(start, stop, f):
        def body(i, carry):
            f(i)
            return carry

        lax.fori_loop(start, stop, body, 0)

    barrier = pltpu.get_barrier_semaphore()

    def greet(**where):
        pl.semaphore_signal(barrier, inc=1, device_id=where, device_id_type=MESH)

    for d in range(1, n_tp):
        greet(tp=tp(d))
        greet(tp=tp(d), sp=mate)
    for d in range(1, reach + 1):
        greet(sp=sp(d))
        greet(sp=sp(-d))

    def load(src, dst, i):
        copy = pltpu.make_async_copy(src, dst, loc.at[i])
        copy.start()
        return copy

    load_cond = load(cond_h, cond, 0)
    load_cond_ctx = load(cond_ctx_h, cond_ctx, 1)
    for kind, matrix in enumerate((w_shift, w_scale, w_gate)):
        load(matrix, wm.at[kind], 2)
    load_lat = load(latent.at[0], lat.at[0], 3)
    load_ctx = load(context.at[0], ctx_rows, 4)
    load(w_key, wkv.at[:, pl.ds(0, HEAD_DIM)], 5)
    load(w_value, wkv.at[:, pl.ds(HEAD_DIM, HEAD_DIM)], 5)
    load_gain = load(norm_gain_h, norm_gain, 6)
    load_key_gain = load(key_gain_h, key_gain, 7)
    load_wq = load(w_query, wq, 8)
    load_query_gain = load(query_gain_h, query_gain, 9)
    load_wo = load(w_out, wo, 10)
    load_out_gain = load(out_gain_h, out_gain, 11)

    def arrived(whole, i):
        pltpu.make_async_copy(whole, whole, loc.at[i]).wait()

    in_rows = wm.shape[1]
    load_cond.wait()
    load_cond_ctx.wait()
    lanes = pl.ds(pl.multiple_of(z * in_rows, in_rows), in_rows)
    own_in = cond[:, lanes].astype(F32)
    every = cond_ctx[...].astype(F32)
    line = lax.broadcasted_iota(jnp.int32, every.shape, 0)
    ctx_in = jnp.sum(jnp.where(line == z, every, 0.0), 0, keepdims=True)
    first_row = lax.broadcasted_iota(jnp.int32, (16, in_rows), 0) == 0
    both = jnp.where(
        first_row,
        jnp.broadcast_to(own_in, (16, in_rows)),
        jnp.broadcast_to(ctx_in, (16, in_rows)),
    )
    activated = jax.nn.silu(both).astype(BF16)
    arrived(wm, 2)
    for kind in range(3):
        product = jnp.dot(activated, wm[kind], preferred_element_type=F32)
        for who in range(2 if kind < 2 else 1):
            for block in range(2):
                for side in range(2):
                    at = (2 * block + side) * 128
                    row = (2 * kind + who) * 2 + side
                    part[block, row : row + 1, :] = product[who : who + 1, at : at + 128]

    load_lat.wait()
    pl.semaphore_wait(barrier, 2 * reach + 2 * (n_tp - 1))

    used = pl.ds(0, 10)
    offsets = [o for i in range(reach, 0, -1) for o in (i, -i) if o > -reach]
    p1 = [
        remote(
            part.at[lax.rem(sp(-o), 2), used],
            got_mod.at[i, used],
            p1_send.at[0],
            p1_recv.at[0],
            sp=sp(-o),
        )
        for i, o in enumerate(offsets)
    ]
    for copy in p1:
        copy.start()

    lo, hi = pl.ds(0, half), pl.ds(half, half)
    x_copies = [
        remote(lat.at[0, lo], lat.at[1, lo], x_send.at[0], x_recv.at[0], tp=tp(1)),
        remote(lat.at[0, hi], lat.at[2, hi], x_send.at[0], x_recv.at[1], tp=tp(-1)),
        remote(lat.at[0, hi], lat.at[1, hi], x_send.at[0], x_recv.at[2], tp=tp(1)),
        remote(lat.at[0, lo], lat.at[2, lo], x_send.at[0], x_recv.at[3], tp=tp(-1)),
        remote(lat.at[1, lo], lat.at[3, lo], x_send.at[0], x_recv.at[4], tp=tp(1)),
        remote(lat.at[2, hi], lat.at[3, hi], x_send.at[0], x_recv.at[4], tp=tp(-1)),
    ]
    for copy in x_copies[:4]:
        copy.start()

    cos_t[0:n_ctx, :] = jnp.ones((n_ctx, HEAD_DIM), F32)
    sin_t[0:n_ctx, :] = jnp.zeros((n_ctx, HEAD_DIM), F32)
    lane = lax.broadcasted_iota(jnp.int32, (tok, HEAD_DIM), 1)
    place = lax.broadcasted_iota(jnp.int32, (tok, HEAD_DIM), 0)
    quarter = HEAD_DIM // 4
    inverse = jnp.exp((lane & (quarter - 1)).astype(F32) * (-math.log(10000.0) / quarter))
    lower = (lane & (2 * quarter - 1)) < quarter
    for j in range(n_tp):
        token = z * seq + tp(RELATIVE[j]) * tok + place
        grid_row = token >> (GRID_WIDTH.bit_length() - 1)
        grid_col = token & (GRID_WIDTH - 1)
        angle = jnp.where(lane < 2 * quarter, grid_row, grid_col).astype(F32) * inverse
        at = n_ctx + j * tok
        cos_t[at : at + tok, :] = jnp.cos(angle)
        sine = jnp.sin(angle)
        sin_t[at : at + tok, :] = jnp.where(lower, -sine, sine)

    def prepare(read, base, count):
        def body(i, carry):
            floats = read(pl.ds(pl.multiple_of(i * 16, 16), 16)).astype(F32)
            inv = lax.rsqrt(jnp.mean(floats * floats, -1, keepdims=True) + EPSILON)
            unit[pl.ds(pl.multiple_of(base + i * 16, 16), 16), :] = floats * inv
            return carry

        lax.fori_loop(0, count // 16, body, 0)

    load_ctx.wait()
    prepare(lambda i: ctx_rows[i, :], 0, n_ctx)
    prepare(lambda i: lat[0, i, :], n_ctx, tok)
    arrived(wkv, 5)
    load_gain.wait()
    load_key_gain.wait()

    every_got = got_mod.at[:, used]
    remote(every_got, every_got, p1_send.at[0], p1_recv.at[0], sp=mate).wait_recv()
    window[...] = sum((got_mod[i, 0:10, :] for i in range(len(p1))), part[parity, 0:10, :])
    halves = [
        remote(window, got_half.at[i], h_send.at[0], h_recv.at[i], sp=sp(d))
        for i, d in enumerate((reach, -reach))
    ]
    for copy in halves:
        copy.start()
    for copy in halves:
        copy.wait_recv()
    own_mod[...] = got_half[0] + got_half[1]
    mod_all[x, parity, 0:10, :] = own_mod[...]
    spread = [(d, e) for e in (1, 0) for d in (2, 1, 3, 0) if (d, e) != (0, 0)]
    p2 = []
    for i, (d, e) in enumerate(spread):
        where = {}
        if d:
            where["tp"] = tp(d)
        if e:
            where["sp"] = mate
        p2.append(
            remote(own_mod, mod_all.at[x, parity, used], p2_send.at[0], p2_recv.at[i], **where)
        )
    for copy in p2:
        copy.start()

    x_copies[0].wait_recv()
    x_copies[4].start()
    x_copies[1].wait_recv()
    x_copies[5].start()
    x_copies[2].wait_recv()
    prepare(lambda i: lat[1, i, :], n_ctx + tok, tok)
    x_copies[3].wait_recv()
    prepare(lambda i: lat[2, i, :], n_ctx + 2 * tok, tok)
    for copy in p2:
        copy.wait_recv()

    cols = width // n_tp
    for b in range(n_tp):
        for block in range(2):
            tile = mod_all[b, block, 0:10, :]
            for side in range(2):
                at = b * cols + (2 * block + side) * 128
                gain = norm_gain[:, at : at + 128]
                for who in range(2):
                    r = who * 2 + side
                    rows_mod[who : who + 1, at : at + 128] = tile[r : r + 1, :]
                    rows_mod[2 + who : 3 + who, at : at + 128] = gain * (
                        1.0 + tile[4 + r : 5 + r, :]
                    )
                rows_mod[4:5, at : at + 128] = tile[8 + side : 9 + side, :]

    def norm_rows(base, count, who):
        shift = rows_mod[who : who + 1, :]
        scale = rows_mod[2 + who : 3 + who, :]

        def body(i, carry):
            at = pl.ds(pl.multiple_of(base + i * 16, 16), 16)
            normed[at, :] = (unit[at, :] * scale + shift).astype(BF16)
            return carry

        lax.fori_loop(0, count // 16, body, 0)

    def head_norm(raw, gain):
        floats = raw.astype(BF16).astype(F32)
        return floats * lax.rsqrt(jnp.mean(floats * floats, -1, keepdims=True) + EPSILON) * gain

    def rotate(vectors, at, count):
        d = lax.broadcasted_iota(jnp.int32, (count, HEAD_DIM), 1)
        swapped = jnp.where(
            (d & (2 * quarter - 1)) < quarter,
            pltpu.roll(vectors, HEAD_DIM - quarter, 1),
            pltpu.roll(vectors, quarter, 1),
        )
        return vectors * cos_t[at : at + count, :] + swapped * sin_t[at : at + count, :]

    bounds = [(0, n_ctx + tok)] + [(n_ctx + j * tok, tok) for j in range(1, n_tp)]

    def ring(way, slot, j, final=False):
        at, count = bounds[j]
        buf = kv_r if way == 0 else kv_l
        piece = pl.ds(at, count)
        target = sp(1) if way == 0 else sp(-1)
        return remote(
            buf.at[slot - 1, :, piece],
            buf.at[slot, :, piece],
            r_send.at[way + 2 if final else way],
            r_recv.at[way, slot - 1, j],
            sp=target,
        )

    norm_rows(0, n_ctx, 1)
    for j in range(n_tp):
        at, count = bounds[j]
        if j == 3:
            remote(lat.at[3], lat.at[3], x_send.at[0], x_recv.at[4], tp=tp(1)).wait_recv()
            prepare(lambda i: lat[3, i, :], n_ctx + 3 * tok, tok)
        norm_rows(n_ctx + j * tok, tok, 0)
        made = jnp.dot(normed[at : at + count, :], wkv[...], preferred_element_type=F32)
        keys = rotate(head_norm(made[:, :HEAD_DIM], key_gain[...]), at, count).astype(BF16)
        values = made[:, HEAD_DIM:].astype(BF16)
        kv_r[0, 0, at : at + count, :] = keys
        kv_l[0, 0, at : at + count, :] = keys
        kv_r[0, 1, at : at + count, :] = values
        kv_l[0, 1, at : at + count, :] = values
        ring(0, 1, j).start()
        ring(1, 1, j).start()

    last = n_sp // 2
    factor = LOG2E * HEAD_DIM ** (-0.5)
    nt = (((1,), (1,)), ((), ()))

    def attend(g, keys, values, first=False, lift_from=None):
        scores = lax.dot_general(q_s[g], keys, nt, preferred_element_type=F32) * factor
        if lift_from is not None:
            lift = (ctx_lift[g] + math.log(seq / n_ctx)) * LOG2E
            at = lax.broadcasted_iota(jnp.int32, (1, keys.shape[0]), 1)
            scores = scores + jnp.where(at >= lift_from, lift, 0.0)
        top = jnp.max(scores, -1, keepdims=True)
        if not first:
            before = m_s[g]
            top = jnp.maximum(before, top)
        weights = jnp.exp2(scores - top)
        total = jnp.sum(weights, -1, keepdims=True)
        out = jnp.dot(weights.astype(BF16), values, preferred_element_type=F32)
        if not first:
            keep = jnp.exp2(before - top)
            total = total + l_s[g] * keep
            out = out + acc_s[g] * keep
        m_s[g] = top
        l_s[g] = total
        acc_s[g] = out

    def pull(s, j):
        for way in range(2):
            short = (j < 2) if way == 0 else (j >= 2)

            def wait(way=way):
                ring(way, s, j).wait_recv()

            def forward(final, way=way):
                ring(way, s + 1, j, final).start()

            if isinstance(s, int):
                if s < last or short:
                    wait()
                if s + 1 < last:
                    forward(False)
                elif s + 1 == last and short:
                    forward(True)
                continue
            wait()
            pl.when(s + 1 < last)(functools.partial(forward, False))
            if short:
                pl.when(s + 1 == last)(functools.partial(forward, True))

    body_rows = pl.ds(n_ctx, seq)
    pull(1, 0)
    load_wq.wait()
    load_query_gain.wait()
    made = jnp.dot(normed[n_ctx:rows, :], wq[...], preferred_element_type=F32)
    for g in range(2):
        q_s[g] = rotate(
            head_norm(made[:, g * HEAD_DIM : (g + 1) * HEAD_DIM], query_gain[...]), n_ctx, seq
        ).astype(BF16)
    pull(1, 1)
    attend(0, kv_r[0, 0, body_rows], kv_r[0, 1, body_rows], first=True)
    pull(1, 2)
    pull(1, 3)
    attend(1, kv_r[0, 0, body_rows], kv_r[0, 1, body_rows], first=True)

    def pair(slot, kind):
        return jnp.concatenate([kv_r[slot, kind, body_rows], kv_l[slot, kind, body_rows]], 0)

    def step(s, carry):
        for g in range(2):
            for j in (2 * g, 2 * g + 1):
                pull(s, j)
            attend(g, pair(s - 1, 0), pair(s - 1, 1))
        return carry

    lax.fori_loop(2, last, step, 0)

    def joined(kind):
        parts = [kv_r[last - 1, kind, body_rows], kv_l[last - 1, kind, body_rows]]
        parts += [kv_r[s, kind, 0:n_ctx] for s in range(last)]
        parts += [kv_l[s, kind, 0:n_ctx] for s in range(1, last)]
        return jnp.concatenate(parts, 0)

    for g in range(2):
        attend(g, joined(0), joined(1), lift_from=2 * seq)

    cut = bounds[2][0]

    def ending(kind):
        parts = [kv_r[last, kind, n_ctx:cut], kv_l[last, kind, cut:rows], kv_r[last, kind, 0:n_ctx]]
        return jnp.concatenate(parts, 0)

    def exchange(g, j):
        part_of = pl.ds(g * HEAD_DIM, HEAD_DIM)
        return remote(
            att_send.at[j, :, part_of],
            att_all.at[x, :, part_of],
            o_send.at[0],
            o_recv.at[j - 1],
            tp=tp(RELATIVE[j]),
        )

    for j in range(n_tp):
        pull(last, j)
    for g in range(2):
        attend(g, ending(0), ending(1), lift_from=seq)
        att = (acc_s[g] / l_s[g]).astype(BF16)
        for j in range(n_tp):
            att_send[j, :, g * HEAD_DIM : (g + 1) * HEAD_DIM] = att[j * tok : (j + 1) * tok]
    for g in range(2):
        for j in (3, 1, 2):
            exchange(g, j).start()
    att_all[x] = att_send[0]
    load_wo.wait()
    load_out_gain.wait()
    for j in range(1, n_tp):
        whole = att_all.at[tp(-RELATIVE[j])]
        remote(whole, whole, o_send.at[0], o_recv.at[j - 1], tp=tp(1)).wait_recv()

    channels = att_all.shape[2]
    pieces = [att_all[b].astype(F32) for b in range(n_tp)]
    square = sum(jnp.sum(p * p, -1, keepdims=True) for p in pieces)
    inv = lax.rsqrt(square * (1.0 / (n_tp * channels)) + EPSILON)
    for b in range(n_tp):
        gain = out_gain[:, b * channels : (b + 1) * channels]
        att_n[:, b * channels : (b + 1) * channels] = (pieces[b] * inv * gain).astype(BF16)
    strip = 512
    for i in range(width // strip):
        at = pl.ds(i * strip, strip)
        mix = jnp.dot(att_n[...], wo[:, at], preferred_element_type=F32)
        result[0, :, at] = (lat[0, :, at].astype(F32) + rows_mod[4:5, at] * mix).astype(BF16)

    def sent(whole, sem):
        remote(whole, whole, sem, p1_recv.at[0], sp=mate).wait_send()

    sent(lat.at[0:3], x_send.at[0])
    sent(every_got, p1_send.at[0])
    sent(got_mod.at[0 : len(p2), used], p2_send.at[0])
    sent(got_half, h_send.at[0])
    sent(kv_r.at[0 : last - 1], r_send.at[0])
    sent(kv_l.at[0 : last - 1], r_send.at[1])
    at, _ = bounds[2]
    sent(kv_r.at[last - 1, :, 0:at], r_send.at[2])
    sent(kv_l.at[last - 1, :, at:rows], r_send.at[3])
    sent(att_send.at[1:n_tp], o_send.at[0])


def on_device(mesh, *args):
    (
        latent,
        cond,
        context,
        cond_ctx,
        w_shift,
        w_scale,
        w_gate,
        norm_gain,
        w_query,
        w_key,
        w_value,
        query_gain,
        key_gain,
        ctx_lift,
        out_gain,
        w_out,
    ) = args
    n_sp, n_tp = mesh.shape["sp"], mesh.shape["tp"]
    assert n_tp == 4 and KV_HEADS == n_tp and n_sp % 4 == 0
    assert w_shift.shape == (128, 512)
    tok, width = latent.shape[1:]
    n_ctx = context.shape[1]
    rows = n_ctx + n_tp * tok
    seq = n_tp * tok
    slots = n_sp // 2 + 1
    any_ = pl.BlockSpec(memory_space=pl.ANY)
    smem = pl.BlockSpec(memory_space=pltpu.SMEM)
    dma = pltpu.SemaphoreType.DMA
    scratch = [
        pltpu.VMEM((1, width), BF16),
        pltpu.VMEM((width // 128, 128), BF16),
        pltpu.VMEM((1, width), F32),
        pltpu.VMEM((1, HEAD_DIM), F32),
        pltpu.VMEM((1, HEAD_DIM), F32),
        pltpu.VMEM((1, HEADS * HEAD_DIM), F32),
        pltpu.VMEM((n_tp, tok, width), BF16),
        pltpu.VMEM((n_ctx, width), BF16),
        pltpu.VMEM((3,) + w_shift.shape, BF16),
        pltpu.VMEM(w_query.shape, BF16),
        pltpu.VMEM((width, 2 * HEAD_DIM), BF16),
        pltpu.VMEM(w_out.shape, BF16),
        pltpu.VMEM((2, 16, 128), F32),
        pltpu.VMEM((n_sp // 2 - 1, 16, 128), F32),
        pltpu.VMEM((10, 128), F32),
        pltpu.VMEM((2, 10, 128), F32),
        pltpu.VMEM((10, 128), F32),
        pltpu.VMEM((n_tp, 2, 16, 128), F32),
        pltpu.VMEM((8, width), F32),
        pltpu.VMEM((rows, width), F32),
        pltpu.VMEM((rows, width), BF16),
        pltpu.VMEM((rows, HEAD_DIM), F32),
        pltpu.VMEM((rows, HEAD_DIM), F32),
        pltpu.VMEM((slots, 2, rows, HEAD_DIM), BF16),
        pltpu.VMEM((slots, 2, rows, HEAD_DIM), BF16),
        pltpu.VMEM((2, seq, HEAD_DIM), BF16),
        pltpu.VMEM((2, seq, 1), F32),
        pltpu.VMEM((2, seq, 1), F32),
        pltpu.VMEM((2, seq, HEAD_DIM), F32),
        pltpu.VMEM((n_tp, tok, 2 * HEAD_DIM), BF16),
        pltpu.VMEM((n_tp, tok, 2 * HEAD_DIM), BF16),
        pltpu.VMEM((tok, HEADS * HEAD_DIM), BF16),
        dma((12,)),
        dma((1,)),
        dma((5,)),
        dma((1,)),
        dma((1,)),
        dma((1,)),
        dma((2,)),
        dma((1,)),
        dma((7,)),
        dma((4,)),
        dma((2, slots - 1, 4)),
        dma((1,)),
        dma((3,)),
    ]
    specs = [any_] * 13 + [smem, any_, any_]
    row = lambda a: a.reshape(1, -1)
    return pl.pallas_call(
        functools.partial(kernel, n_sp),
        out_shape=pltpu.VMEM(latent.shape, BF16),
        in_specs=specs,
        out_specs=pl.BlockSpec(memory_space=pltpu.VMEM),
        scratch_shapes=scratch,
        compiler_params=pltpu.CompilerParams(
            collective_id=0, has_side_effects=True, vmem_limit_bytes=56 << 20
        ),
    )(
        latent,
        cond,
        context,
        cond_ctx.reshape(-1, 128),
        w_shift,
        w_scale,
        w_gate,
        row(norm_gain),
        w_query,
        w_key,
        w_value,
        row(query_gain),
        row(key_gain),
        ctx_lift,
        row(out_gain),
        w_out,
    )


def solution(mesh):
    in_specs = (
        P(("grp", "dp"), ("sp", "tp"), None),
        P(("grp", "dp"), None),
        P(("grp", "dp"), "sp", None),
        P(),
        P("sp", "tp"),
        P("sp", "tp"),
        P("sp", "tp"),
        P(),
        P(None, "tp"),
        P(None, "tp"),
        P(None, "tp"),
        P(),
        P(),
        P("tp"),
        P(),
        P(),
    )
    out_specs = P(("grp", "dp"), ("sp", "tp"), None)
    return jax.shard_map(
        functools.partial(on_device, mesh),
        mesh=mesh,
        in_specs=in_specs,
        out_specs=out_specs,
        check_vma=False,
    )
```

```python
import functools
import math

import jax
import jax.numpy as jnp
from jax import lax
from jax.experimental import pallas as pl
from jax.experimental.pallas import tpu as pltpu
from jax.sharding import PartitionSpec as P

HEADS = 8
KV_HEADS = 4
HEAD_DIM = 128
GRID_WIDTH = 64
EPSILON = 1e-06
LOG2E = math.log2(math.e)
MESH = pl.DeviceIdType.MESH
F32 = jnp.float32
BF16 = jnp.bfloat16
RELATIVE = (0, 3, 1, 2)


def kernel(
    n_sp,
    latent,
    cond_h,
    context,
    cond_ctx_h,
    w_shift,
    w_scale,
    w_gate,
    norm_gain_h,
    w_query,
    w_key,
    w_value,
    query_gain_h,
    key_gain_h,
    ctx_lift,
    out_gain_h,
    w_out,
    result,
    cond,
    cond_ctx,
    norm_gain,
    query_gain,
    key_gain,
    out_gain,
    lat,
    ctx_rows,
    wm,
    wq,
    wkv,
    wo,
    part,
    got_mod,
    window,
    got_half,
    own_mod,
    mod_all,
    rows_mod,
    unit,
    normed,
    cos_t,
    sin_t,
    kv_r,
    kv_l,
    q_s,
    lift_s,
    m_s,
    l_s,
    acc_s,
    att_send,
    att_all,
    att_n,
    loc,
    x_send,
    x_recv,
    p1_send,
    p1_recv,
    h_send,
    h_recv,
    p2_send,
    p2_recv,
    r_send,
    r_recv,
    o_send,
    o_recv,
):
    z = lax.axis_index("sp")
    x = lax.axis_index("tp")
    n_tp = 4
    tok = lat.shape[1]
    half = tok // 2
    n_ctx = ctx_rows.shape[0]
    seq = n_tp * tok
    rows = n_ctx + seq
    width = lat.shape[2]
    reach = n_sp // 4
    mate = z + 1 - 2 * lax.rem(z, 2)
    parity = lax.rem(z, 2)

    def sp(d):
        return lax.rem(z + d + n_sp, n_sp)

    def tp(d):
        return lax.rem(x + d + n_tp, n_tp)

    def remote(src, dst, s, r, **where):
        return pltpu.make_async_remote_copy(
            src_ref=src,
            dst_ref=dst,
            send_sem=s,
            recv_sem=r,
            device_id=where,
            device_id_type=MESH,
        )

    def each(start, stop, f):
        def body(i, carry):
            f(i)
            return carry

        lax.fori_loop(start, stop, body, 0)

    barrier = pltpu.get_barrier_semaphore()

    def greet(**where):
        pl.semaphore_signal(barrier, inc=1, device_id=where, device_id_type=MESH)

    for d in range(1, n_tp):
        greet(tp=tp(d))
        greet(tp=tp(d), sp=mate)
    for d in range(1, reach + 1):
        greet(sp=sp(d))
        greet(sp=sp(-d))

    def load(src, dst, i):
        copy = pltpu.make_async_copy(src, dst, loc.at[i])
        copy.start()
        return copy

    load_cond = load(cond_h, cond, 0)
    load_cond_ctx = load(cond_ctx_h, cond_ctx, 1)
    for kind, matrix in enumerate((w_shift, w_scale, w_gate)):
        load(matrix, wm.at[kind], 2)
    load_lat = load(latent.at[0], lat.at[0], 3)
    load_ctx = load(context.at[0], ctx_rows, 4)
    load(w_key, wkv.at[:, pl.ds(0, HEAD_DIM)], 5)
    load(w_value, wkv.at[:, pl.ds(HEAD_DIM, HEAD_DIM)], 5)
    load_gain = load(norm_gain_h, norm_gain, 6)
    load_key_gain = load(key_gain_h, key_gain, 7)
    load_wq = load(w_query, wq, 8)
    load_query_gain = load(query_gain_h, query_gain, 9)
    load_wo = load(w_out, wo, 10)
    load_out_gain = load(out_gain_h, out_gain, 11)

    def arrived(whole, i):
        pltpu.make_async_copy(whole, whole, loc.at[i]).wait()

    in_rows = wm.shape[1]
    load_cond.wait()
    load_cond_ctx.wait()
    lanes = pl.ds(pl.multiple_of(z * in_rows, in_rows), in_rows)
    own_in = cond[:, lanes].astype(F32)
    every = cond_ctx[...].astype(F32)
    line = lax.broadcasted_iota(jnp.int32, every.shape, 0)
    ctx_in = jnp.sum(jnp.where(line == z, every, 0.0), 0, keepdims=True)
    first_row = lax.broadcasted_iota(jnp.int32, (16, in_rows), 0) == 0
    both = jnp.where(
        first_row,
        jnp.broadcast_to(own_in, (16, in_rows)),
        jnp.broadcast_to(ctx_in, (16, in_rows)),
    )
    activated = jax.nn.silu(both).astype(BF16)
    arrived(wm, 2)
    for kind in range(3):
        product = jnp.dot(activated, wm[kind], preferred_element_type=F32)
        for who in range(2 if kind < 2 else 1):
            for block in range(2):
                for side in range(2):
                    at = (2 * block + side) * 128
                    row = (2 * kind + who) * 2 + side
                    part[block, row : row + 1, :] = product[who : who + 1, at : at + 128]

    load_lat.wait()
    pl.semaphore_wait(barrier, 2 * reach + 2 * (n_tp - 1))

    used = pl.ds(0, 10)
    offsets = [o for i in range(reach, 0, -1) for o in (i, -i) if o > -reach]
    p1 = [
        remote(
            part.at[lax.rem(sp(-o), 2), used],
            got_mod.at[i, used],
            p1_send.at[0],
            p1_recv.at[0],
            sp=sp(-o),
        )
        for i, o in enumerate(offsets)
    ]
    for copy in p1:
        copy.start()

    lo, hi = pl.ds(0, half), pl.ds(half, half)
    x_copies = [
        remote(lat.at[0, lo], lat.at[1, lo], x_send.at[0], x_recv.at[0], tp=tp(1)),
        remote(lat.at[0, hi], lat.at[2, hi], x_send.at[0], x_recv.at[1], tp=tp(-1)),
        remote(lat.at[0, hi], lat.at[1, hi], x_send.at[0], x_recv.at[2], tp=tp(1)),
        remote(lat.at[0, lo], lat.at[2, lo], x_send.at[0], x_recv.at[3], tp=tp(-1)),
        remote(lat.at[1, lo], lat.at[3, lo], x_send.at[0], x_recv.at[4], tp=tp(1)),
        remote(lat.at[2, hi], lat.at[3, hi], x_send.at[0], x_recv.at[4], tp=tp(-1)),
    ]
    for copy in x_copies[:4]:
        copy.start()

    cos_t[0:n_ctx, :] = jnp.ones((n_ctx, HEAD_DIM), F32)
    sin_t[0:n_ctx, :] = jnp.zeros((n_ctx, HEAD_DIM), F32)
    lane = lax.broadcasted_iota(jnp.int32, (tok, HEAD_DIM), 1)
    place = lax.broadcasted_iota(jnp.int32, (tok, HEAD_DIM), 0)
    quarter = HEAD_DIM // 4
    inverse = jnp.exp((lane & (quarter - 1)).astype(F32) * (-math.log(10000.0) / quarter))
    lower = (lane & (2 * quarter - 1)) < quarter
    for j in range(n_tp):
        token = z * seq + tp(RELATIVE[j]) * tok + place
        grid_row = token >> (GRID_WIDTH.bit_length() - 1)
        grid_col = token & (GRID_WIDTH - 1)
        angle = jnp.where(lane < 2 * quarter, grid_row, grid_col).astype(F32) * inverse
        at = n_ctx + j * tok
        cos_t[at : at + tok, :] = jnp.cos(angle)
        sine = jnp.sin(angle)
        sin_t[at : at + tok, :] = jnp.where(lower, -sine, sine)

    for g in range(2):
        lift = (ctx_lift[g] + math.log(seq / n_ctx)) * LOG2E
        for j in range(n_tp):
            lift_s[pl.ds((2 * j + g) * tok, tok)] = jnp.full((tok, 1), lift, F32)

    def prepare(read, base, count):
        def body(i, carry):
            floats = read(pl.ds(pl.multiple_of(i * 16, 16), 16)).astype(F32)
            inv = lax.rsqrt(jnp.mean(floats * floats, -1, keepdims=True) + EPSILON)
            unit[pl.ds(pl.multiple_of(base + i * 16, 16), 16), :] = floats * inv
            return carry

        lax.fori_loop(0, count // 16, body, 0)

    load_ctx.wait()
    prepare(lambda i: ctx_rows[i, :], 0, n_ctx)
    prepare(lambda i: lat[0, i, :], n_ctx, tok)
    arrived(wkv, 5)
    load_gain.wait()
    load_key_gain.wait()

    every_got = got_mod.at[:, used]
    remote(every_got, every_got, p1_send.at[0], p1_recv.at[0], sp=mate).wait_recv()
    window[...] = sum((got_mod[i, 0:10, :] for i in range(len(p1))), part[parity, 0:10, :])
    halves = [
        remote(window, got_half.at[i], h_send.at[0], h_recv.at[i], sp=sp(d))
        for i, d in enumerate((reach, -reach))
    ]
    for copy in halves:
        copy.start()
    for copy in halves:
        copy.wait_recv()
    own_mod[...] = got_half[0] + got_half[1]
    mod_all[x, parity, 0:10, :] = own_mod[...]
    spread = [(d, e) for e in (1, 0) for d in (2, 1, 3, 0) if (d, e) != (0, 0)]
    p2 = []
    for i, (d, e) in enumerate(spread):
        where = {}
        if d:
            where["tp"] = tp(d)
        if e:
            where["sp"] = mate
        p2.append(
            remote(own_mod, mod_all.at[x, parity, used], p2_send.at[0], p2_recv.at[i], **where)
        )
    for copy in p2:
        copy.start()

    x_copies[0].wait_recv()
    x_copies[4].start()
    x_copies[1].wait_recv()
    x_copies[5].start()
    x_copies[2].wait_recv()
    prepare(lambda i: lat[1, i, :], n_ctx + tok, tok)
    x_copies[3].wait_recv()
    prepare(lambda i: lat[2, i, :], n_ctx + 2 * tok, tok)
    for copy in p2:
        copy.wait_recv()

    cols = width // n_tp
    for b in range(n_tp):
        for block in range(2):
            tile = mod_all[b, block, 0:10, :]
            for side in range(2):
                at = b * cols + (2 * block + side) * 128
                gain = norm_gain[:, at : at + 128]
                for who in range(2):
                    r = who * 2 + side
                    rows_mod[who : who + 1, at : at + 128] = tile[r : r + 1, :]
                    rows_mod[2 + who : 3 + who, at : at + 128] = gain * (
                        1.0 + tile[4 + r : 5 + r, :]
                    )
                rows_mod[4:5, at : at + 128] = tile[8 + side : 9 + side, :]

    def norm_rows(base, count, who):
        shift = rows_mod[who : who + 1, :]
        scale = rows_mod[2 + who : 3 + who, :]

        def body(i, carry):
            at = pl.ds(pl.multiple_of(base + i * 16, 16), 16)
            normed[at, :] = (unit[at, :] * scale + shift).astype(BF16)
            return carry

        lax.fori_loop(0, count // 16, body, 0)

    def head_norm(raw, gain):
        floats = raw.astype(BF16).astype(F32)
        return floats * lax.rsqrt(jnp.mean(floats * floats, -1, keepdims=True) + EPSILON) * gain

    def rotate(vectors, at, count):
        d = lax.broadcasted_iota(jnp.int32, (count, HEAD_DIM), 1)
        swapped = jnp.where(
            (d & (2 * quarter - 1)) < quarter,
            pltpu.roll(vectors, HEAD_DIM - quarter, 1),
            pltpu.roll(vectors, quarter, 1),
        )
        return vectors * cos_t[at : at + count, :] + swapped * sin_t[at : at + count, :]

    bounds = [(0, n_ctx + tok)] + [(n_ctx + j * tok, tok) for j in range(1, n_tp)]

    def ring(way, slot, j, final=False):
        at, count = bounds[j]
        buf = kv_r if way == 0 else kv_l
        piece = pl.ds(at, count)
        target = sp(1) if way == 0 else sp(-1)
        return remote(
            buf.at[slot - 1, :, piece],
            buf.at[slot, :, piece],
            r_send.at[way + 2 if final else way],
            r_recv.at[way, slot - 1, j],
            sp=target,
        )

    norm_rows(0, n_ctx, 1)
    for j in range(n_tp):
        at, count = bounds[j]
        if j == 3:
            remote(lat.at[3], lat.at[3], x_send.at[0], x_recv.at[4], tp=tp(1)).wait_recv()
            prepare(lambda i: lat[3, i, :], n_ctx + 3 * tok, tok)
        norm_rows(n_ctx + j * tok, tok, 0)
        made = jnp.dot(normed[at : at + count, :], wkv[...], preferred_element_type=F32)
        keys = rotate(head_norm(made[:, :HEAD_DIM], key_gain[...]), at, count).astype(BF16)
        values = made[:, HEAD_DIM:].astype(BF16)
        kv_r[0, 0, at : at + count, :] = keys
        kv_l[0, 0, at : at + count, :] = keys
        kv_r[0, 1, at : at + count, :] = values
        kv_l[0, 1, at : at + count, :] = values
        ring(0, 1, j).start()
        ring(1, 1, j).start()

    last = n_sp // 2
    factor = LOG2E * HEAD_DIM ** (-0.5)
    nt = (((1,), (1,)), ((), ()))

    def attend(at, count, keys, values, extra=None, first=False, final=False):
        here = pl.ds(at, count)
        queries = q_s[here]
        scores = lax.dot_general(queries, keys, nt, preferred_element_type=F32) * factor
        if extra is not None:
            more = lax.dot_general(queries, extra[0], nt, preferred_element_type=F32) * factor
            scores = jnp.concatenate([scores, more + lift_s[here]], 1)
            values = jnp.concatenate([values, extra[1]], 0)
        top = jnp.max(scores, -1, keepdims=True)
        if not first:
            before = m_s[here]
            top = jnp.maximum(before, top)
        weights = jnp.exp2(scores - top)
        full = weights.shape[1] // 128 * 128
        total = sum(weights[:, i : i + 128] for i in range(0, full, 128))
        if full < weights.shape[1]:
            rest = jnp.sum(weights[:, full:], -1, keepdims=True)
            one = lax.broadcasted_iota(jnp.int32, total.shape, 1) == 0
            total = total + jnp.where(one, rest, 0.0)
        out = jnp.dot(weights.astype(BF16), values, preferred_element_type=F32)
        if not first:
            keep = jnp.exp2(before - top)
            total = total + l_s[here] * keep
            out = out + acc_s[here] * keep
        if final:
            return (out / jnp.sum(total, -1, keepdims=True)).astype(BF16)
        m_s[here] = top
        l_s[here] = total
        acc_s[here] = out

    def pull(s, j):
        for way in range(2):
            short = (j < 2) if way == 0 else (j >= 2)

            def wait(way=way):
                ring(way, s, j).wait_recv()

            def forward(final, way=way):
                ring(way, s + 1, j, final).start()

            if isinstance(s, int):
                if s < last or short:
                    wait()
                if s + 1 < last:
                    forward(False)
                elif s + 1 == last and short:
                    forward(True)
                continue
            wait()
            pl.when(s + 1 < last)(functools.partial(forward, False))
            if short:
                pl.when(s + 1 == last)(functools.partial(forward, True))

    body_rows = pl.ds(n_ctx, seq)
    pull(1, 0)
    load_wq.wait()
    load_query_gain.wait()
    made = jnp.dot(normed[n_ctx:rows, :], wq[...], preferred_element_type=F32)
    for g in range(2):
        turned = rotate(
            head_norm(made[:, g * HEAD_DIM : (g + 1) * HEAD_DIM], query_gain[...]), n_ctx, seq
        ).astype(BF16)
        for j in range(n_tp):
            q_s[pl.ds((2 * j + g) * tok, tok)] = turned[j * tok : (j + 1) * tok]
    pull(1, 1)
    for part_of in range(2):
        attend(part_of * seq, seq, kv_r[0, 0, body_rows], kv_r[0, 1, body_rows], first=True)
    pull(1, 2)
    pull(1, 3)

    def both(slot, kind):
        return jnp.concatenate([kv_r[slot, kind, body_rows], kv_l[slot, kind, body_rows]], 0)

    def step(s, carry):
        for part_of in range(2):
            pull(s, 2 * part_of)
            pull(s, 2 * part_of + 1)
            attend(part_of * seq, seq, both(s - 1, 0), both(s - 1, 1))
        return carry

    lax.fori_loop(2, last, step, 0)

    def contexts(kind):
        parts = [kv_r[s, kind, 0:n_ctx] for s in range(last)]
        parts += [kv_l[s, kind, 0:n_ctx] for s in range(1, last)]
        return jnp.concatenate(parts, 0)

    for part_of in range(2):
        attend(
            part_of * seq,
            seq,
            both(last - 1, 0),
            both(last - 1, 1),
            extra=(contexts(0), contexts(1)),
        )

    cut = bounds[2][0]

    def ending(kind):
        return jnp.concatenate([kv_r[last, kind, n_ctx:cut], kv_l[last, kind, cut:rows]], 0)

    for j in range(n_tp):
        pull(last, j)
    sends = []
    for j in (3, 1, 2, 0):
        att = attend(
            2 * j * tok,
            2 * tok,
            ending(0),
            ending(1),
            extra=(kv_r[last, 0, 0:n_ctx], kv_r[last, 1, 0:n_ctx]),
            final=True,
        )
        for g in range(2):
            half_att = att[g * tok : (g + 1) * tok]
            if j == 0:
                att_all[x, :, pl.ds(g * HEAD_DIM, HEAD_DIM)] = half_att
            else:
                att_send[j - 1, :, pl.ds(g * HEAD_DIM, HEAD_DIM)] = half_att
        if j > 0:
            copy = remote(
                att_send.at[j - 1],
                att_all.at[x],
                o_send.at[0],
                o_recv.at[j - 1],
                tp=tp(RELATIVE[j]),
            )
            copy.start()
    load_wo.wait()
    load_out_gain.wait()

    def channel_block(b):
        floats = att_all[b].astype(F32)
        return jnp.sum(floats * floats, -1, keepdims=True)

    square = channel_block(x)
    for j in (1, 2, 3):
        source = tp(-RELATIVE[j])
        whole = att_all.at[source]
        remote(whole, whole, o_send.at[0], o_recv.at[j - 1], tp=tp(1)).wait_recv()
        square = square + channel_block(source)

    channels = att_all.shape[2]
    inv = lax.rsqrt(square * (1.0 / (n_tp * channels)) + EPSILON)
    for b in range(n_tp):
        gain = out_gain[:, b * channels : (b + 1) * channels]
        att_n[:, b * channels : (b + 1) * channels] = (
            att_all[b].astype(F32) * inv * gain
        ).astype(BF16)
    strip = 512
    for i in range(width // strip):
        at = pl.ds(i * strip, strip)
        mix = jnp.dot(att_n[...], wo[:, at], preferred_element_type=F32)
        result[0, :, at] = (lat[0, :, at].astype(F32) + rows_mod[4:5, at] * mix).astype(BF16)

    def sent(whole, sem):
        remote(whole, whole, sem, p1_recv.at[0], sp=mate).wait_send()

    sent(lat.at[0:3], x_send.at[0])
    sent(every_got, p1_send.at[0])
    sent(got_mod.at[0 : len(p2), used], p2_send.at[0])
    sent(got_half, h_send.at[0])
    sent(kv_r.at[0 : last - 1], r_send.at[0])
    sent(kv_l.at[0 : last - 1], r_send.at[1])
    at, _ = bounds[2]
    sent(kv_r.at[last - 1, :, 0:at], r_send.at[2])
    sent(kv_l.at[last - 1, :, at:rows], r_send.at[3])
    sent(att_send, o_send.at[0])


def on_device(mesh, *args):
    (
        latent,
        cond,
        context,
        cond_ctx,
        w_shift,
        w_scale,
        w_gate,
        norm_gain,
        w_query,
        w_key,
        w_value,
        query_gain,
        key_gain,
        ctx_lift,
        out_gain,
        w_out,
    ) = args
    n_sp, n_tp = mesh.shape["sp"], mesh.shape["tp"]
    assert n_tp == 4 and KV_HEADS == n_tp and n_sp % 4 == 0
    assert w_shift.shape == (128, 512)
    tok, width = latent.shape[1:]
    n_ctx = context.shape[1]
    rows = n_ctx + n_tp * tok
    seq = n_tp * tok
    slots = n_sp // 2 + 1
    any_ = pl.BlockSpec(memory_space=pl.ANY)
    smem = pl.BlockSpec(memory_space=pltpu.SMEM)
    dma = pltpu.SemaphoreType.DMA
    scratch = [
        pltpu.VMEM((1, width), BF16),
        pltpu.VMEM((width // 128, 128), BF16),
        pltpu.VMEM((1, width), F32),
        pltpu.VMEM((1, HEAD_DIM), F32),
        pltpu.VMEM((1, HEAD_DIM), F32),
        pltpu.VMEM((1, HEADS * HEAD_DIM), F32),
        pltpu.VMEM((n_tp, tok, width), BF16),
        pltpu.VMEM((n_ctx, width), BF16),
        pltpu.VMEM((3,) + w_shift.shape, BF16),
        pltpu.VMEM(w_query.shape, BF16),
        pltpu.VMEM((width, 2 * HEAD_DIM), BF16),
        pltpu.VMEM(w_out.shape, BF16),
        pltpu.VMEM((2, 16, 128), F32),
        pltpu.VMEM((n_sp // 2 - 1, 16, 128), F32),
        pltpu.VMEM((10, 128), F32),
        pltpu.VMEM((2, 10, 128), F32),
        pltpu.VMEM((10, 128), F32),
        pltpu.VMEM((n_tp, 2, 16, 128), F32),
        pltpu.VMEM((8, width), F32),
        pltpu.VMEM((rows, width), F32),
        pltpu.VMEM((rows, width), BF16),
        pltpu.VMEM((rows, HEAD_DIM), F32),
        pltpu.VMEM((rows, HEAD_DIM), F32),
        pltpu.VMEM((slots, 2, rows, HEAD_DIM), BF16),
        pltpu.VMEM((slots, 2, rows, HEAD_DIM), BF16),
        pltpu.VMEM((2 * seq, HEAD_DIM), BF16),
        pltpu.VMEM((2 * seq, 1), F32),
        pltpu.VMEM((2 * seq, 1), F32),
        pltpu.VMEM((2 * seq, 128), F32),
        pltpu.VMEM((2 * seq, HEAD_DIM), F32),
        pltpu.VMEM((n_tp - 1, tok, 2 * HEAD_DIM), BF16),
        pltpu.VMEM((n_tp, tok, 2 * HEAD_DIM), BF16),
        pltpu.VMEM((tok, HEADS * HEAD_DIM), BF16),
        dma((12,)),
        dma((1,)),
        dma((5,)),
        dma((1,)),
        dma((1,)),
        dma((1,)),
        dma((2,)),
        dma((1,)),
        dma((7,)),
        dma((4,)),
        dma((2, slots - 1, 4)),
        dma((1,)),
        dma((3,)),
    ]
    specs = [any_] * 13 + [smem, any_, any_]
    row = lambda a: a.reshape(1, -1)
    return pl.pallas_call(
        functools.partial(kernel, n_sp),
        out_shape=pltpu.VMEM(latent.shape, BF16),
        in_specs=specs,
        out_specs=pl.BlockSpec(memory_space=pltpu.VMEM),
        scratch_shapes=scratch,
        compiler_params=pltpu.CompilerParams(
            collective_id=0, has_side_effects=True, vmem_limit_bytes=56 << 20
        ),
    )(
        latent,
        cond,
        context,
        cond_ctx.reshape(-1, 128),
        w_shift,
        w_scale,
        w_gate,
        row(norm_gain),
        w_query,
        w_key,
        w_value,
        row(query_gain),
        row(key_gain),
        ctx_lift,
        row(out_gain),
        w_out,
    )


def solution(mesh):
    in_specs = (
        P(("grp", "dp"), ("sp", "tp"), None),
        P(("grp", "dp"), None),
        P(("grp", "dp"), "sp", None),
        P(),
        P("sp", "tp"),
        P("sp", "tp"),
        P("sp", "tp"),
        P(),
        P(None, "tp"),
        P(None, "tp"),
        P(None, "tp"),
        P(),
        P(),
        P("tp"),
        P(),
        P(),
    )
    out_specs = P(("grp", "dp"), ("sp", "tp"), None)
    return jax.shard_map(
        functools.partial(on_device, mesh),
        mesh=mesh,
        in_specs=in_specs,
        out_specs=out_specs,
        check_vma=False,
    )
```

```python
import functools
import math

import jax
import jax.numpy as jnp
from jax import lax
from jax.experimental import pallas as pl
from jax.experimental.pallas import tpu as pltpu
from jax.sharding import PartitionSpec as P

HEADS = 8
KV_HEADS = 4
HEAD_DIM = 128
GRID_WIDTH = 64
EPSILON = 1e-06
LOG2E = math.log2(math.e)
MESH = pl.DeviceIdType.MESH
F32 = jnp.float32
BF16 = jnp.bfloat16
RELATIVE = (0, 3, 1, 2)


def kernel(
    n_sp,
    latent,
    cond_h,
    context,
    cond_ctx_h,
    w_shift,
    w_scale,
    w_gate,
    norm_gain_h,
    w_query,
    w_key,
    w_value,
    query_gain_h,
    key_gain_h,
    ctx_lift,
    out_gain_h,
    w_out,
    result,
    cond,
    cond_ctx,
    norm_gain,
    query_gain,
    key_gain,
    out_gain,
    lat,
    ctx_rows,
    wm,
    wq,
    wkv,
    wo,
    part,
    both_got,
    window,
    got_half,
    own_mod,
    mod_all,
    rows_mod,
    unit,
    normed,
    cos_t,
    sin_t,
    kv_r,
    kv_l,
    q_s,
    lift_s,
    m_s,
    l_s,
    acc_s,
    att_send,
    att_all,
    att_n,
    loc,
    x_send,
    x_recv,
    p1_send,
    p1_recv,
    h_send,
    h_recv,
    p2_send,
    p2_recv,
    r_send,
    r_recv,
    o_send,
    o_recv,
):
    z = lax.axis_index("sp")
    x = lax.axis_index("tp")
    core = lax.axis_index("dp")
    n_tp = 4
    tok = lat.shape[1]
    half = tok // 2
    n_ctx = ctx_rows.shape[0]
    seq = n_tp * tok
    rows = n_ctx + seq
    width = lat.shape[2]
    reach = n_sp // 4
    got_mod = both_got.at[0 : n_sp // 2 - 1]
    got_other = both_got.at[n_sp // 2 - 1 : n_sp - 1]
    mate = z + 1 - 2 * lax.rem(z, 2)
    parity = lax.rem(z, 2)

    def sp(d):
        return lax.rem(z + d + n_sp, n_sp)

    def tp(d):
        return lax.rem(x + d + n_tp, n_tp)

    def remote(src, dst, s, r, **where):
        return pltpu.make_async_remote_copy(
            src_ref=src,
            dst_ref=dst,
            send_sem=s,
            recv_sem=r,
            device_id=where,
            device_id_type=MESH,
        )

    def each(start, stop, f):
        def body(i, carry):
            f(i)
            return carry

        lax.fori_loop(start, stop, body, 0)

    barrier = pltpu.get_barrier_semaphore()

    def greet(**where):
        pl.semaphore_signal(barrier, inc=1, device_id=where, device_id_type=MESH)

    for d in range(reach, 0, -1):
        greet(sp=sp(d), dp=1)
        greet(sp=sp(-d), dp=1)
    for d in (2, 1, 3):
        greet(tp=tp(d), sp=mate, dp=1)
        greet(tp=tp(d), dp=1)

    @pl.when(core == 0)
    def _():
        greet(sp=sp(1))
        greet(sp=sp(-1))
        for d in range(1, n_tp):
            greet(tp=tp(d))
        greet(dp=1)

    @pl.when(core == 1)
    def _():
        for d in range(reach, 0, -1):
            greet(sp=sp(d), dp=0)
            greet(sp=sp(-d), dp=0)
        for d in (2, 1, 3):
            greet(tp=tp(d), sp=mate, dp=0)
            greet(tp=tp(d), dp=0)
        greet(dp=0)

    common = 2 * reach + 2 * (n_tp - 1)
    greeted = jnp.where(core == 0, common + 2 + n_tp, 2 * common + 1)

    def load(src, dst, i):
        copy = pltpu.make_async_copy(src, dst, loc.at[i])
        copy.start()
        return copy

    load_cond = load(cond_h, cond, 0)
    load_cond_ctx = load(cond_ctx_h, cond_ctx, 1)
    for kind, matrix in enumerate((w_shift, w_scale, w_gate)):
        load(matrix, wm.at[kind], 2)
    load_lat = load(latent.at[0], lat.at[0], 3)
    load_ctx = load(context.at[0], ctx_rows, 4)
    load(w_key, wkv.at[:, pl.ds(0, HEAD_DIM)], 5)
    load(w_value, wkv.at[:, pl.ds(HEAD_DIM, HEAD_DIM)], 5)
    load_gain = load(norm_gain_h, norm_gain, 6)
    load_key_gain = load(key_gain_h, key_gain, 7)
    load_wq = load(w_query, wq, 8)
    load_query_gain = load(query_gain_h, query_gain, 9)
    load_wo = load(w_out, wo, 10)
    load_out_gain = load(out_gain_h, out_gain, 11)

    def arrived(whole, i):
        pltpu.make_async_copy(whole, whole, loc.at[i]).wait()

    in_rows = wm.shape[1]
    load_cond.wait()
    load_cond_ctx.wait()
    lanes = pl.ds(pl.multiple_of(z * in_rows, in_rows), in_rows)
    own_in = cond[:, lanes].astype(F32)
    every = cond_ctx[...].astype(F32)
    line = lax.broadcasted_iota(jnp.int32, every.shape, 0)
    ctx_in = jnp.sum(jnp.where(line == z, every, 0.0), 0, keepdims=True)
    first_row = lax.broadcasted_iota(jnp.int32, (16, in_rows), 0) == 0
    both = jnp.where(
        first_row,
        jnp.broadcast_to(own_in, (16, in_rows)),
        jnp.broadcast_to(ctx_in, (16, in_rows)),
    )
    activated = jax.nn.silu(both).astype(BF16)
    arrived(wm, 2)
    for kind in range(3):
        product = jnp.dot(activated, wm[kind], preferred_element_type=F32)
        for who in range(2 if kind < 2 else 1):
            for block in range(2):
                for side in range(2):
                    at = (2 * block + side) * 128
                    row = (2 * kind + who) * 2 + side
                    part[block, row : row + 1, :] = product[who : who + 1, at : at + 128]

    load_lat.wait()
    pl.semaphore_wait(barrier, greeted)

    used = pl.ds(0, 10)
    offsets = [o for i in range(reach, 0, -1) for o in (i, -i) if o > -reach]

    def p1(own, i, o):
        return remote(
            part.at[lax.rem(sp(-o), 2), used],
            (got_mod if own else got_other).at[i, used],
            p1_send.at[0],
            p1_recv.at[0 if own else 1],
            sp=sp(-o),
            dp=1,
        )

    @pl.when(core == 1)
    def _():
        for i, o in enumerate(offsets):
            p1(True, i, o).start()

    @pl.when(core == 0)
    def _():
        for i, o in enumerate(offsets + [0]):
            p1(False, i, o).start()

    lo, hi = pl.ds(0, half), pl.ds(half, half)
    x_copies = [
        remote(lat.at[0, lo], lat.at[1, lo], x_send.at[0], x_recv.at[0], tp=tp(1)),
        remote(lat.at[0, hi], lat.at[2, hi], x_send.at[0], x_recv.at[1], tp=tp(-1)),
        remote(lat.at[0, hi], lat.at[1, hi], x_send.at[0], x_recv.at[2], tp=tp(1)),
        remote(lat.at[0, lo], lat.at[2, lo], x_send.at[0], x_recv.at[3], tp=tp(-1)),
        remote(lat.at[1, lo], lat.at[3, lo], x_send.at[0], x_recv.at[4], tp=tp(1)),
        remote(lat.at[2, hi], lat.at[3, hi], x_send.at[0], x_recv.at[4], tp=tp(-1)),
    ]
    for copy in x_copies[:4]:
        copy.start()

    cos_t[0:n_ctx, :] = jnp.ones((n_ctx, HEAD_DIM), F32)
    sin_t[0:n_ctx, :] = jnp.zeros((n_ctx, HEAD_DIM), F32)
    lane = lax.broadcasted_iota(jnp.int32, (tok, HEAD_DIM), 1)
    place = lax.broadcasted_iota(jnp.int32, (tok, HEAD_DIM), 0)
    quarter = HEAD_DIM // 4
    inverse = jnp.exp((lane & (quarter - 1)).astype(F32) * (-math.log(10000.0) / quarter))
    lower = (lane & (2 * quarter - 1)) < quarter
    for j in range(n_tp):
        token = z * seq + tp(RELATIVE[j]) * tok + place
        grid_row = token >> (GRID_WIDTH.bit_length() - 1)
        grid_col = token & (GRID_WIDTH - 1)
        angle = jnp.where(lane < 2 * quarter, grid_row, grid_col).astype(F32) * inverse
        at = n_ctx + j * tok
        cos_t[at : at + tok, :] = jnp.cos(angle)
        sine = jnp.sin(angle)
        sin_t[at : at + tok, :] = jnp.where(lower, -sine, sine)

    for g in range(2):
        lift = (ctx_lift[g] + math.log(seq / n_ctx)) * LOG2E
        for j in range(n_tp):
            lift_s[pl.ds((2 * j + g) * tok, tok)] = jnp.full((tok, 1), lift, F32)

    def prepare(read, base, count):
        def body(i, carry):
            floats = read(pl.ds(pl.multiple_of(i * 16, 16), 16)).astype(F32)
            inv = lax.rsqrt(jnp.mean(floats * floats, -1, keepdims=True) + EPSILON)
            unit[pl.ds(pl.multiple_of(base + i * 16, 16), 16), :] = floats * inv
            return carry

        lax.fori_loop(0, count // 16, body, 0)

    load_ctx.wait()
    prepare(lambda i: ctx_rows[i, :], 0, n_ctx)
    prepare(lambda i: lat[0, i, :], n_ctx, tok)
    arrived(wkv, 5)
    load_gain.wait()
    load_key_gain.wait()

    own_got = got_mod.at[:, used]
    other_got = got_other.at[:, used]

    def half_window(own, i):
        return remote(
            window.at[0 if own else 1],
            got_half.at[i if own else 2 + i],
            h_send.at[0],
            h_recv.at[i if own else 2 + i],
            sp=sp((reach, -reach)[i]),
        )

    spread = [(d, e) for e in (1, 0) for d in (2, 1, 3, 0)]

    def p2(core_of, i):
        d, e = spread[i]
        where = dict(dp=core_of)
        if d:
            where["tp"] = tp(d)
        if e:
            where["sp"] = mate
        return remote(
            own_mod.at[1 - core_of],
            mod_all.at[x, parity, used],
            p2_send.at[0],
            p2_recv.at[i],
            **where,
        )

    @pl.when(core == 1)
    def _():
        remote(own_got, own_got, p1_send.at[0], p1_recv.at[0], sp=mate).wait_recv()
        window[0] = sum((got_mod[i, 0:10, :] for i in range(len(offsets))), part[parity, 0:10, :])
        for i in range(2):
            half_window(True, i).start()
        remote(other_got, other_got, p1_send.at[0], p1_recv.at[1], sp=mate).wait_recv()
        window[1] = sum(got_other[i, 0:10, :] for i in range(len(offsets) + 1))
        for i in range(2):
            half_window(False, i).start()
        for i in range(2):
            half_window(True, i).wait_recv()
        own_mod[0] = got_half[0] + got_half[1]
        mod_all[x, parity, 0:10, :] = own_mod[0]
        for i in range(7):
            p2(1, i).start()
        for i in range(2):
            half_window(False, i).wait_recv()
        own_mod[1] = got_half[2] + got_half[3]
        for i in range(8):
            p2(0, i).start()

    x_copies[0].wait_recv()
    x_copies[4].start()
    x_copies[1].wait_recv()
    x_copies[5].start()
    prepare(lambda i: lat[1, i, :], n_ctx + tok, half)
    prepare(lambda i: lat[2, pl.ds(half + i.start, i.size), :], n_ctx + 2 * tok + half, half)
    for i in range(7):
        p2(1, i).wait_recv()

    @pl.when(core == 0)
    def _():
        p2(0, 7).wait_recv()


    cols = width // n_tp
    for b in range(n_tp):
        for block in range(2):
            tile = mod_all[b, block, 0:10, :]
            for side in range(2):
                at = b * cols + (2 * block + side) * 128
                gain = norm_gain[:, at : at + 128]
                for who in range(2):
                    r = who * 2 + side
                    rows_mod[who : who + 1, at : at + 128] = tile[r : r + 1, :]
                    rows_mod[2 + who : 3 + who, at : at + 128] = gain * (
                        1.0 + tile[4 + r : 5 + r, :]
                    )
                rows_mod[4:5, at : at + 128] = tile[8 + side : 9 + side, :]

    def norm_rows(base, count, who):
        shift = rows_mod[who : who + 1, :]
        scale = rows_mod[2 + who : 3 + who, :]

        def body(i, carry):
            at = pl.ds(pl.multiple_of(base + i * 16, 16), 16)
            normed[at, :] = (unit[at, :] * scale + shift).astype(BF16)
            return carry

        lax.fori_loop(0, count // 16, body, 0)

    def head_norm(raw, gain):
        floats = raw.astype(BF16).astype(F32)
        return floats * lax.rsqrt(jnp.mean(floats * floats, -1, keepdims=True) + EPSILON) * gain

    def rotate(vectors, pieces):
        d = lax.broadcasted_iota(jnp.int32, vectors.shape, 1)
        cosine = jnp.concatenate([cos_t[b : b + n, :] for b, n in pieces], 0)
        sine = jnp.concatenate([sin_t[b : b + n, :] for b, n in pieces], 0)
        swapped = jnp.where(
            (d & (2 * quarter - 1)) < quarter,
            pltpu.roll(vectors, HEAD_DIM - quarter, 1),
            pltpu.roll(vectors, quarter, 1),
        )
        return vectors * cosine + swapped * sine

    second, third = n_ctx + tok, n_ctx + 2 * tok
    chunk_rows = [
        [(0, n_ctx + tok)],
        [(second, half), (third + half, half)],
        [(second + half, half), (third, half)],
        [(n_ctx + 3 * tok, tok)],
    ]

    bounds = [(0, n_ctx + tok)] + [(n_ctx + j * tok, tok) for j in range(1, n_tp)]

    def ring(way, slot, j, final=False):
        at, count = bounds[j]
        buf = kv_r if way == 0 else kv_l
        piece = pl.ds(at, count)
        target = sp(1) if way == 0 else sp(-1)
        return remote(
            buf.at[slot - 1, :, piece],
            buf.at[slot, :, piece],
            r_send.at[way + 2 if final else way],
            r_recv.at[way, slot - 1, j],
            sp=target,
        )

    last = n_sp // 2
    factor = LOG2E * HEAD_DIM ** (-0.5)
    nt = (((1,), (1,)), ((), ()))

    def attend(at, count, keys, values, extra=None, first=False, final=False):
        here = pl.ds(at, count)
        queries = q_s[here]
        scores = lax.dot_general(queries, keys, nt, preferred_element_type=F32) * factor
        if extra is not None:
            more = lax.dot_general(queries, extra[0], nt, preferred_element_type=F32) * factor
            scores = jnp.concatenate([scores, more + lift_s[here]], 1)
            values = jnp.concatenate([values, extra[1]], 0)
        top = jnp.broadcast_to(jnp.max(scores, -1, keepdims=True), (count, 128))
        if not first:
            before = m_s[here]
            top = jnp.maximum(before, top)
        size = scores.shape[1]
        wide = jnp.concatenate([top] * (size // 128) + [top[:, : size % 128]] * (size % 128 > 0), 1)
        weights = jnp.exp2(scores - wide)
        full = weights.shape[1] // 128 * 128
        total = sum(weights[:, i : i + 128] for i in range(0, full, 128))
        if full < weights.shape[1]:
            rest = jnp.sum(weights[:, full:], -1, keepdims=True)
            one = lax.broadcasted_iota(jnp.int32, total.shape, 1) == 0
            total = total + jnp.where(one, rest, 0.0)
        out = jnp.dot(weights.astype(BF16), values, preferred_element_type=F32)
        if not first:
            keep = jnp.exp2(before - top)
            total = total + l_s[here] * keep
            out = out + acc_s[here] * keep
        if final:
            return (out / jnp.sum(total, -1, keepdims=True)).astype(BF16)
        m_s[here] = top
        l_s[here] = total
        acc_s[here] = out

    def pull(s, j):
        for way in range(2):
            short = (j < 2) if way == 0 else (j >= 2)

            def wait(way=way):
                ring(way, s, j).wait_recv()

            def forward(final, way=way):
                ring(way, s + 1, j, final).start()

            if isinstance(s, int):
                if s < last or short:
                    wait()
                if s + 1 < last:
                    forward(False)
                elif s + 1 == last and short:
                    forward(True)
                continue
            wait()
            pl.when(s + 1 < last)(functools.partial(forward, False))
            if short:
                pl.when(s + 1 == last)(functools.partial(forward, True))

    norm_rows(0, n_ctx, 1)
    norm_rows(n_ctx, tok, 0)

    def produce(j):
        at, count = bounds[j]
        if j == 2:
            x_copies[2].wait_recv()
            x_copies[3].wait_recv()
            prepare(lambda i: lat[1, pl.ds(half + i.start, i.size), :], second + half, half)
            prepare(lambda i: lat[2, i, :], third, half)
        if j == 3:
            remote(lat.at[3], lat.at[3], x_send.at[0], x_recv.at[4], tp=tp(1)).wait_recv()
            prepare(lambda i: lat[3, i, :], n_ctx + 3 * tok, tok)
        pieces = chunk_rows[j]
        if j > 0:
            for begin, size in pieces:
                norm_rows(begin, size, 0)
        inputs = jnp.concatenate([normed[b : b + n, :] for b, n in pieces], 0)
        made = jnp.dot(inputs, wkv[...], preferred_element_type=F32)
        keys = rotate(head_norm(made[:, :HEAD_DIM], key_gain[...]), pieces).astype(BF16)
        values = made[:, HEAD_DIM:].astype(BF16)
        kv_r[0, 0, at : at + count, :] = keys
        kv_l[0, 0, at : at + count, :] = keys
        kv_r[0, 1, at : at + count, :] = values
        kv_l[0, 1, at : at + count, :] = values
        ring(0, 1, j).start()
        ring(1, 1, j).start()

    body_rows = pl.ds(n_ctx, seq)
    produce(0)
    produce(1)
    produce(2)
    pull(1, 0)
    produce(3)
    pull(1, 1)
    load_wq.wait()
    load_query_gain.wait()
    made = jnp.dot(normed[n_ctx:rows, :], wq[...], preferred_element_type=F32)
    for g in range(2):
        turned = rotate(
            head_norm(made[:, g * HEAD_DIM : (g + 1) * HEAD_DIM], query_gain[...]), [(n_ctx, seq)]
        ).astype(BF16)
        for j in range(n_tp):
            q_s[pl.ds((2 * j + g) * tok, tok)] = turned[j * tok : (j + 1) * tok]
    pull(1, 2)
    for part_of in range(2):
        attend(part_of * seq, seq, kv_r[0, 0, body_rows], kv_r[0, 1, body_rows], first=True)

    def both(slot, kind):
        return jnp.concatenate([kv_r[slot, kind, body_rows], kv_l[slot, kind, body_rows]], 0)

    def step(s, carry):
        for part_of in range(2):
            if part_of == 0:
                pull(s, 0)
                pull(s - 1, 3)
            else:
                pull(s, 1)
                pull(s, 2)
            attend(part_of * seq, seq, both(s - 1, 0), both(s - 1, 1))
        return carry

    lax.fori_loop(2, last, step, 0)
    pull(last, 0)
    pull(last - 1, 3)

    def contexts(kind):
        parts = [kv_r[s, kind, 0:n_ctx] for s in range(last)]
        parts += [kv_l[s, kind, 0:n_ctx] for s in range(1, last)]
        return jnp.concatenate(parts, 0)

    for part_of in range(2):
        attend(
            part_of * seq,
            seq,
            both(last - 1, 0),
            both(last - 1, 1),
            extra=(contexts(0), contexts(1)),
        )

    cut = bounds[2][0]

    def ending(kind):
        return jnp.concatenate([kv_r[last, kind, n_ctx:cut], kv_l[last, kind, cut:rows]], 0)

    for j in range(1, n_tp):
        pull(last, j)
    sends = []
    for j in (3, 1, 2, 0):
        att = attend(
            2 * j * tok,
            2 * tok,
            ending(0),
            ending(1),
            extra=(kv_r[last, 0, 0:n_ctx], kv_r[last, 1, 0:n_ctx]),
            final=True,
        )
        for g in range(2):
            half_att = att[g * tok : (g + 1) * tok]
            if j == 0:
                att_all[x, :, pl.ds(g * HEAD_DIM, HEAD_DIM)] = half_att
            else:
                att_send[j - 1, :, pl.ds(g * HEAD_DIM, HEAD_DIM)] = half_att
        if j > 0:
            copy = remote(
                att_send.at[j - 1],
                att_all.at[x],
                o_send.at[0],
                o_recv.at[j - 1],
                tp=tp(RELATIVE[j]),
            )
            copy.start()
    load_wo.wait()
    load_out_gain.wait()

    def channel_block(b):
        floats = att_all[b].astype(F32)
        return jnp.sum(floats * floats, -1, keepdims=True)

    square = channel_block(x)
    for j in (1, 2, 3):
        source = tp(-RELATIVE[j])
        whole = att_all.at[source]
        remote(whole, whole, o_send.at[0], o_recv.at[j - 1], tp=tp(1)).wait_recv()
        square = square + channel_block(source)

    channels = att_all.shape[2]
    inv = lax.rsqrt(square * (1.0 / (n_tp * channels)) + EPSILON)
    for b in range(n_tp):
        gain = out_gain[:, b * channels : (b + 1) * channels]
        att_n[:, b * channels : (b + 1) * channels] = (
            att_all[b].astype(F32) * inv * gain
        ).astype(BF16)
    strip = 512
    for i in range(width // strip):
        at = pl.ds(i * strip, strip)
        mix = jnp.dot(att_n[...], wo[:, at], preferred_element_type=F32)
        result[0, :, at] = (lat[0, :, at].astype(F32) + rows_mod[4:5, at] * mix).astype(BF16)

    def sent(whole, sem):
        remote(whole, whole, sem, p1_recv.at[0], sp=mate).wait_send()

    sent(lat.at[0:3], x_send.at[0])

    @pl.when(core == 0)
    def _():
        sent(other_got, p1_send.at[0])

    @pl.when(core == 1)
    def _():
        sent(own_got, p1_send.at[0])
        sent(got_half, h_send.at[0])
        sent(both_got.at[:, used], p2_send.at[0])

    sent(kv_r.at[0 : last - 1], r_send.at[0])
    sent(kv_l.at[0 : last - 1], r_send.at[1])
    at, _ = bounds[2]
    sent(kv_r.at[last - 1, :, 0:at], r_send.at[2])
    sent(kv_l.at[last - 1, :, at:rows], r_send.at[3])
    sent(att_send, o_send.at[0])


def on_device(mesh, *args):
    (
        latent,
        cond,
        context,
        cond_ctx,
        w_shift,
        w_scale,
        w_gate,
        norm_gain,
        w_query,
        w_key,
        w_value,
        query_gain,
        key_gain,
        ctx_lift,
        out_gain,
        w_out,
    ) = args
    n_sp, n_tp = mesh.shape["sp"], mesh.shape["tp"]
    assert mesh.shape["dp"] == 2
    assert n_tp == 4 and KV_HEADS == n_tp and n_sp == 16
    assert w_shift.shape == (128, 512)
    tok, width = latent.shape[1:]
    n_ctx = context.shape[1]
    rows = n_ctx + n_tp * tok
    seq = n_tp * tok
    slots = n_sp // 2 + 1
    any_ = pl.BlockSpec(memory_space=pl.ANY)
    smem = pl.BlockSpec(memory_space=pltpu.SMEM)
    dma = pltpu.SemaphoreType.DMA
    scratch = [
        pltpu.VMEM((1, width), BF16),
        pltpu.VMEM((width // 128, 128), BF16),
        pltpu.VMEM((1, width), F32),
        pltpu.VMEM((1, HEAD_DIM), F32),
        pltpu.VMEM((1, HEAD_DIM), F32),
        pltpu.VMEM((1, HEADS * HEAD_DIM), F32),
        pltpu.VMEM((n_tp, tok, width), BF16),
        pltpu.VMEM((n_ctx, width), BF16),
        pltpu.VMEM((3,) + w_shift.shape, BF16),
        pltpu.VMEM(w_query.shape, BF16),
        pltpu.VMEM((width, 2 * HEAD_DIM), BF16),
        pltpu.VMEM(w_out.shape, BF16),
        pltpu.VMEM((2, 16, 128), F32),
        pltpu.VMEM((n_sp - 1, 16, 128), F32),
        pltpu.VMEM((2, 10, 128), F32),
        pltpu.VMEM((4, 10, 128), F32),
        pltpu.VMEM((2, 10, 128), F32),
        pltpu.VMEM((n_tp, 2, 16, 128), F32),
        pltpu.VMEM((8, width), F32),
        pltpu.VMEM((rows, width), F32),
        pltpu.VMEM((rows, width), BF16),
        pltpu.VMEM((rows, HEAD_DIM), F32),
        pltpu.VMEM((rows, HEAD_DIM), F32),
        pltpu.VMEM((slots, 2, rows, HEAD_DIM), BF16),
        pltpu.VMEM((slots, 2, rows, HEAD_DIM), BF16),
        pltpu.VMEM((2 * seq, HEAD_DIM), BF16),
        pltpu.VMEM((2 * seq, 1), F32),
        pltpu.VMEM((2 * seq, 128), F32),
        pltpu.VMEM((2 * seq, 128), F32),
        pltpu.VMEM((2 * seq, HEAD_DIM), F32),
        pltpu.VMEM((n_tp - 1, tok, 2 * HEAD_DIM), BF16),
        pltpu.VMEM((n_tp, tok, 2 * HEAD_DIM), BF16),
        pltpu.VMEM((tok, HEADS * HEAD_DIM), BF16),
        dma((12,)),
        dma((1,)),
        dma((5,)),
        dma((1,)),
        dma((2,)),
        dma((1,)),
        dma((4,)),
        dma((1,)),
        dma((8,)),
        dma((4,)),
        dma((2, slots - 1, 4)),
        dma((1,)),
        dma((3,)),
    ]
    specs = [any_] * 13 + [smem, any_, any_]
    row = lambda a: a.reshape(1, -1)
    return pl.pallas_call(
        functools.partial(kernel, n_sp),
        out_shape=pltpu.VMEM(latent.shape, BF16),
        in_specs=specs,
        out_specs=pl.BlockSpec(memory_space=pltpu.VMEM),
        scratch_shapes=scratch,
        compiler_params=pltpu.CompilerParams(
            collective_id=0, has_side_effects=True, vmem_limit_bytes=56 << 20
        ),
    )(
        latent,
        cond,
        context,
        cond_ctx.reshape(-1, 128),
        w_shift,
        w_scale,
        w_gate,
        row(norm_gain),
        w_query,
        w_key,
        w_value,
        row(query_gain),
        row(key_gain),
        ctx_lift,
        row(out_gain),
        w_out,
    )


def solution(mesh):
    in_specs = (
        P(("grp", "dp"), ("sp", "tp"), None),
        P(("grp", "dp"), None),
        P(("grp", "dp"), "sp", None),
        P(),
        P("sp", "tp"),
        P("sp", "tp"),
        P("sp", "tp"),
        P(),
        P(None, "tp"),
        P(None, "tp"),
        P(None, "tp"),
        P(),
        P(),
        P("tp"),
        P(),
        P(),
    )
    out_specs = P(("grp", "dp"), ("sp", "tp"), None)
    return jax.shard_map(
        functools.partial(on_device, mesh),
        mesh=mesh,
        in_specs=in_specs,
        out_specs=out_specs,
        check_vma=False,
    )
```

```python
import functools
import math

import jax
import jax.numpy as jnp
from jax import lax
from jax.experimental import pallas as pl
from jax.experimental.pallas import tpu as pltpu
from jax.sharding import PartitionSpec as P

HEADS = 8
KV_HEADS = 4
HEAD_DIM = 128
GRID_WIDTH = 64
EPSILON = 1e-06
LOG2E = math.log2(math.e)
MESH = pl.DeviceIdType.MESH
F32 = jnp.float32
BF16 = jnp.bfloat16
RELATIVE = (0, 3, 1, 2)


def kernel(
    n_sp,
    latent,
    cond_h,
    context,
    cond_ctx_h,
    w_shift,
    w_scale,
    w_gate,
    norm_gain_h,
    w_query,
    w_key,
    w_value,
    query_gain_h,
    key_gain_h,
    ctx_lift,
    out_gain_h,
    w_out,
    result,
    cond,
    cond_ctx,
    norm_gain,
    query_gain,
    key_gain,
    out_gain,
    lat,
    ctx_rows,
    wm,
    wq,
    wkv,
    wo,
    part,
    both_got,
    window,
    got_half,
    own_mod,
    mod_all,
    rows_mod,
    unit,
    normed,
    cos_t,
    sin_t,
    kv_r,
    kv_l,
    q_s,
    lift_s,
    m_s,
    l_s,
    acc_s,
    att_send,
    att_all,
    att_n,
    loc,
    x_send,
    x_recv,
    p1_send,
    p1_recv,
    h_send,
    h_recv,
    p2_send,
    p2_recv,
    r_send,
    r_recv,
    o_send,
    o_recv,
):
    z = lax.axis_index("sp")
    x = lax.axis_index("tp")
    core = lax.axis_index("dp")
    n_tp = 4
    tok = lat.shape[1]
    half = tok // 2
    n_ctx = ctx_rows.shape[0]
    seq = n_tp * tok
    rows = n_ctx + seq
    width = lat.shape[2]
    reach = n_sp // 4
    got_mod = both_got.at[0 : n_sp // 2 - 1]
    got_other = both_got.at[n_sp // 2 - 1 : n_sp - 1]
    mate = z + 1 - 2 * lax.rem(z, 2)
    parity = lax.rem(z, 2)

    def sp(d):
        return lax.rem(z + d + n_sp, n_sp)

    def tp(d):
        return lax.rem(x + d + n_tp, n_tp)

    def remote(src, dst, s, r, **where):
        return pltpu.make_async_remote_copy(
            src_ref=src,
            dst_ref=dst,
            send_sem=s,
            recv_sem=r,
            device_id=where,
            device_id_type=MESH,
        )

    def each(start, stop, f):
        def body(i, carry):
            f(i)
            return carry

        lax.fori_loop(start, stop, body, 0)

    barrier = pltpu.get_barrier_semaphore()

    def greet(**where):
        pl.semaphore_signal(barrier, inc=1, device_id=where, device_id_type=MESH)

    @pl.when(core == 0)
    def _():
        for d in range(reach, 0, -1):
            greet(sp=sp(d), dp=1)
            greet(sp=sp(-d), dp=1)
        greet(dp=1)
        for d in (2, 1, 3):
            greet(tp=tp(d))
            greet(tp=tp(d), dp=1)
            greet(tp=tp(d), sp=mate, dp=1)
        greet(sp=sp(1))
        greet(sp=sp(-1))

    @pl.when(core == 1)
    def _():
        for d in range(reach, 0, -1):
            for to in range(2):
                greet(sp=sp(d), dp=to)
                greet(sp=sp(-d), dp=to)
        greet(dp=0)
        for d in (2, 1, 3):
            for to in (1, 0):
                greet(tp=tp(d), dp=to)
                greet(tp=tp(d), sp=mate, dp=to)

    common = 2 * reach + 2 * (n_tp - 1)
    greeted = jnp.where(core == 0, common + 2 + n_tp, 2 * common + 1)

    def load(src, dst, i):
        copy = pltpu.make_async_copy(src, dst, loc.at[i])
        copy.start()
        return copy

    load_cond = load(cond_h, cond, 0)
    load_cond_ctx = load(cond_ctx_h, cond_ctx, 1)
    for kind, matrix in enumerate((w_shift, w_scale, w_gate)):
        load(matrix, wm.at[kind], 2)
    load_lat = load(latent.at[0], lat.at[0], 3)
    load_ctx = load(context.at[0], ctx_rows, 4)
    load(w_key, wkv.at[:, pl.ds(0, HEAD_DIM)], 5)
    load(w_value, wkv.at[:, pl.ds(HEAD_DIM, HEAD_DIM)], 5)
    load_gain = load(norm_gain_h, norm_gain, 6)
    load_key_gain = load(key_gain_h, key_gain, 7)
    load_wq = load(w_query, wq, 8)
    load_query_gain = load(query_gain_h, query_gain, 9)
    load_wo = load(w_out, wo, 10)
    load_out_gain = load(out_gain_h, out_gain, 11)

    def arrived(whole, i):
        pltpu.make_async_copy(whole, whole, loc.at[i]).wait()

    in_rows = wm.shape[1]
    load_cond.wait()
    load_cond_ctx.wait()
    lanes = pl.ds(pl.multiple_of(z * in_rows, in_rows), in_rows)
    own_in = cond[:, lanes].astype(F32)
    every = cond_ctx[...].astype(F32)
    line = lax.broadcasted_iota(jnp.int32, every.shape, 0)
    ctx_in = jnp.sum(jnp.where(line == z, every, 0.0), 0, keepdims=True)
    first_row = lax.broadcasted_iota(jnp.int32, (16, in_rows), 0) == 0
    both = jnp.where(
        first_row,
        jnp.broadcast_to(own_in, (16, in_rows)),
        jnp.broadcast_to(ctx_in, (16, in_rows)),
    )
    activated = jax.nn.silu(both).astype(BF16)
    arrived(wm, 2)
    for kind in range(3):
        product = jnp.dot(activated, wm[kind], preferred_element_type=F32)
        for who in range(2 if kind < 2 else 1):
            for block in range(2):
                for side in range(2):
                    at = (2 * block + side) * 128
                    row = (2 * kind + who) * 2 + side
                    part[block, row : row + 1, :] = product[who : who + 1, at : at + 128]

    load_lat.wait()
    pl.semaphore_wait(barrier, greeted)

    used = pl.ds(0, 10)
    offsets = [o for i in range(reach, 0, -1) for o in (i, -i) if o > -reach]

    def p1(own, i, o):
        return remote(
            part.at[lax.rem(sp(-o), 2), used],
            (got_mod if own else got_other).at[i, used],
            p1_send.at[0],
            p1_recv.at[0 if own else 1],
            sp=sp(-o),
            dp=1,
        )

    @pl.when(core == 1)
    def _():
        for i, o in enumerate(offsets):
            p1(True, i, o).start()

    @pl.when(core == 0)
    def _():
        for i, o in enumerate(offsets + [0]):
            p1(False, i, o).start()

    lo, hi = pl.ds(0, half), pl.ds(half, half)
    x_copies = [
        remote(lat.at[0, lo], lat.at[1, lo], x_send.at[0], x_recv.at[0], tp=tp(1)),
        remote(lat.at[0, hi], lat.at[2, hi], x_send.at[0], x_recv.at[1], tp=tp(-1)),
        remote(lat.at[0, hi], lat.at[1, hi], x_send.at[0], x_recv.at[2], tp=tp(1)),
        remote(lat.at[0, lo], lat.at[2, lo], x_send.at[0], x_recv.at[3], tp=tp(-1)),
        remote(lat.at[1, lo], lat.at[3, lo], x_send.at[0], x_recv.at[4], tp=tp(1)),
        remote(lat.at[2, hi], lat.at[3, hi], x_send.at[0], x_recv.at[4], tp=tp(-1)),
    ]
    for copy in x_copies[:4]:
        copy.start()

    cos_t[0:n_ctx, :] = jnp.ones((n_ctx, HEAD_DIM), F32)
    sin_t[0:n_ctx, :] = jnp.zeros((n_ctx, HEAD_DIM), F32)
    lane = lax.broadcasted_iota(jnp.int32, (tok, HEAD_DIM), 1)
    place = lax.broadcasted_iota(jnp.int32, (tok, HEAD_DIM), 0)
    quarter = HEAD_DIM // 4
    inverse = jnp.exp((lane & (quarter - 1)).astype(F32) * (-math.log(10000.0) / quarter))
    lower = (lane & (2 * quarter - 1)) < quarter
    for j in range(n_tp):
        token = z * seq + tp(RELATIVE[j]) * tok + place
        grid_row = token >> (GRID_WIDTH.bit_length() - 1)
        grid_col = token & (GRID_WIDTH - 1)
        angle = jnp.where(lane < 2 * quarter, grid_row, grid_col).astype(F32) * inverse
        at = n_ctx + j * tok
        cos_t[at : at + tok, :] = jnp.cos(angle)
        sine = jnp.sin(angle)
        sin_t[at : at + tok, :] = jnp.where(lower, -sine, sine)

    for g in range(2):
        lift = (ctx_lift[g] + math.log(seq / n_ctx)) * LOG2E
        for j in range(n_tp):
            lift_s[pl.ds((2 * j + g) * tok, tok)] = jnp.full((tok, 1), lift, F32)

    def prepare(read, base, count):
        def body(i, carry):
            floats = read(pl.ds(pl.multiple_of(i * 16, 16), 16)).astype(F32)
            inv = lax.rsqrt(jnp.mean(floats * floats, -1, keepdims=True) + EPSILON)
            unit[pl.ds(pl.multiple_of(base + i * 16, 16), 16), :] = floats * inv
            return carry

        lax.fori_loop(0, count // 16, body, 0)

    load_ctx.wait()
    prepare(lambda i: ctx_rows[i, :], 0, n_ctx)
    prepare(lambda i: lat[0, i, :], n_ctx, tok)
    arrived(wkv, 5)
    load_gain.wait()
    load_key_gain.wait()

    own_got = got_mod.at[:, used]
    other_got = got_other.at[:, used]

    def half_window(own, i):
        return remote(
            window.at[0 if own else 1],
            got_half.at[i if own else 2 + i],
            h_send.at[0],
            h_recv.at[i if own else 2 + i],
            sp=sp((reach, -reach)[i]),
        )

    spread = [(d, e) for e in (1, 0) for d in (2, 1, 3, 0)]

    def p2(core_of, i):
        d, e = spread[i]
        where = dict(dp=core_of)
        if d:
            where["tp"] = tp(d)
        if e:
            where["sp"] = mate
        return remote(
            own_mod.at[1 - core_of],
            mod_all.at[x, parity, used],
            p2_send.at[0],
            p2_recv.at[i],
            **where,
        )

    @pl.when(core == 1)
    def _():
        remote(own_got, own_got, p1_send.at[0], p1_recv.at[0], sp=mate).wait_recv()
        window[0] = sum((got_mod[i, 0:10, :] for i in range(len(offsets))), part[parity, 0:10, :])
        for i in range(2):
            half_window(True, i).start()
        remote(other_got, other_got, p1_send.at[0], p1_recv.at[1], sp=mate).wait_recv()
        window[1] = sum(got_other[i, 0:10, :] for i in range(len(offsets) + 1))
        for i in range(2):
            half_window(False, i).start()
        for i in range(2):
            half_window(True, i).wait_recv()
        own_mod[0] = got_half[0] + got_half[1]
        mod_all[x, parity, 0:10, :] = own_mod[0]
        for i in range(7):
            p2(1, i).start()
        for i in range(2):
            half_window(False, i).wait_recv()
        own_mod[1] = got_half[2] + got_half[3]
        for i in range(8):
            p2(0, i).start()

    x_copies[0].wait_recv()
    x_copies[4].start()
    x_copies[1].wait_recv()
    x_copies[5].start()
    prepare(lambda i: lat[1, i, :], n_ctx + tok, half)
    prepare(lambda i: lat[2, pl.ds(half + i.start, i.size), :], n_ctx + 2 * tok + half, half)
    for i in range(7):
        p2(1, i).wait_recv()

    @pl.when(core == 0)
    def _():
        p2(0, 7).wait_recv()


    cols = width // n_tp
    for b in range(n_tp):
        for block in range(2):
            tile = mod_all[b, block, 0:10, :]
            for side in range(2):
                at = b * cols + (2 * block + side) * 128
                gain = norm_gain[:, at : at + 128]
                for who in range(2):
                    r = who * 2 + side
                    rows_mod[who : who + 1, at : at + 128] = tile[r : r + 1, :]
                    rows_mod[2 + who : 3 + who, at : at + 128] = gain * (
                        1.0 + tile[4 + r : 5 + r, :]
                    )
                rows_mod[4:5, at : at + 128] = tile[8 + side : 9 + side, :]

    def norm_rows(base, count, who):
        shift = rows_mod[who : who + 1, :]
        scale = rows_mod[2 + who : 3 + who, :]

        def body(i, carry):
            at = pl.ds(pl.multiple_of(base + i * 16, 16), 16)
            normed[at, :] = (unit[at, :] * scale + shift).astype(BF16)
            return carry

        lax.fori_loop(0, count // 16, body, 0)

    def head_norm(raw, gain):
        floats = raw.astype(BF16).astype(F32)
        return floats * lax.rsqrt(jnp.mean(floats * floats, -1, keepdims=True) + EPSILON) * gain

    def rotate(vectors, pieces):
        d = lax.broadcasted_iota(jnp.int32, vectors.shape, 1)
        cosine = jnp.concatenate([cos_t[b : b + n, :] for b, n in pieces], 0)
        sine = jnp.concatenate([sin_t[b : b + n, :] for b, n in pieces], 0)
        swapped = jnp.where(
            (d & (2 * quarter - 1)) < quarter,
            pltpu.roll(vectors, HEAD_DIM - quarter, 1),
            pltpu.roll(vectors, quarter, 1),
        )
        return vectors * cosine + swapped * sine

    second, third = n_ctx + tok, n_ctx + 2 * tok
    chunk_rows = [
        [(0, n_ctx + tok)],
        [(second, half), (third + half, half)],
        [(second + half, half), (third, half)],
        [(n_ctx + 3 * tok, tok)],
    ]

    bounds = [(0, n_ctx + tok)] + [(n_ctx + j * tok, tok) for j in range(1, n_tp)]

    def ring(way, slot, j, final=False):
        at, count = bounds[j]
        buf = kv_r if way == 0 else kv_l
        piece = pl.ds(at, count)
        target = sp(1) if way == 0 else sp(-1)
        return remote(
            buf.at[slot - 1, :, piece],
            buf.at[slot, :, piece],
            r_send.at[way + 2 if final else way],
            r_recv.at[way, slot - 1, j],
            sp=target,
        )

    last = n_sp // 2
    factor = LOG2E * HEAD_DIM ** (-0.5)
    nt = (((1,), (1,)), ((), ()))

    def attend(at, count, keys, values, extra=None, first=False, final=False):
        here = pl.ds(at, count)
        queries = q_s[here]
        scores = lax.dot_general(queries, keys, nt, preferred_element_type=F32) * factor
        if extra is not None:
            more = lax.dot_general(queries, extra[0], nt, preferred_element_type=F32) * factor
            scores = jnp.concatenate([scores, more + lift_s[here]], 1)
            values = jnp.concatenate([values, extra[1]], 0)
        top = jnp.broadcast_to(jnp.max(scores, -1, keepdims=True), (count, 128))
        if not first:
            before = m_s[here]
            top = jnp.maximum(before, top)
        size = scores.shape[1]
        wide = jnp.concatenate([top] * (size // 128) + [top[:, : size % 128]] * (size % 128 > 0), 1)
        weights = jnp.exp2(scores - wide)
        full = weights.shape[1] // 128 * 128
        total = sum(weights[:, i : i + 128] for i in range(0, full, 128))
        if full < weights.shape[1]:
            rest = jnp.sum(weights[:, full:], -1, keepdims=True)
            one = lax.broadcasted_iota(jnp.int32, total.shape, 1) == 0
            total = total + jnp.where(one, rest, 0.0)
        out = jnp.dot(weights.astype(BF16), values, preferred_element_type=F32)
        if not first:
            keep = jnp.exp2(before - top)
            total = total + l_s[here] * keep
            out = out + acc_s[here] * keep
        if final:
            return (out / jnp.sum(total, -1, keepdims=True)).astype(BF16)
        m_s[here] = top
        l_s[here] = total
        acc_s[here] = out

    def pull(s, j):
        for way in range(2):
            short = (j < 2) if way == 0 else (j >= 2)

            def wait(way=way):
                ring(way, s, j).wait_recv()

            def forward(final, way=way):
                ring(way, s + 1, j, final).start()

            if isinstance(s, int):
                if s < last or short:
                    wait()
                if s + 1 < last:
                    forward(False)
                elif s + 1 == last and short:
                    forward(True)
                continue
            wait()
            pl.when(s + 1 < last)(functools.partial(forward, False))
            if short:
                pl.when(s + 1 == last)(functools.partial(forward, True))

    norm_rows(0, n_ctx, 1)
    norm_rows(n_ctx, tok, 0)

    def produce(j):
        at, count = bounds[j]
        if j == 2:
            x_copies[2].wait_recv()
            x_copies[3].wait_recv()
            prepare(lambda i: lat[1, pl.ds(half + i.start, i.size), :], second + half, half)
            prepare(lambda i: lat[2, i, :], third, half)
        if j == 3:
            remote(lat.at[3], lat.at[3], x_send.at[0], x_recv.at[4], tp=tp(1)).wait_recv()
            prepare(lambda i: lat[3, i, :], n_ctx + 3 * tok, tok)
        pieces = chunk_rows[j]
        if j > 0:
            for begin, size in pieces:
                norm_rows(begin, size, 0)
        inputs = jnp.concatenate([normed[b : b + n, :] for b, n in pieces], 0)
        made = jnp.dot(inputs, wkv[...], preferred_element_type=F32)
        keys = rotate(head_norm(made[:, :HEAD_DIM], key_gain[...]), pieces).astype(BF16)
        values = made[:, HEAD_DIM:].astype(BF16)
        kv_r[0, 0, at : at + count, :] = keys
        kv_l[0, 0, at : at + count, :] = keys
        kv_r[0, 1, at : at + count, :] = values
        kv_l[0, 1, at : at + count, :] = values
        ring(0, 1, j).start()
        ring(1, 1, j).start()

    body_rows = pl.ds(n_ctx, seq)
    produce(0)
    produce(1)
    produce(2)
    pull(1, 0)
    produce(3)
    pull(1, 1)
    load_wq.wait()
    load_query_gain.wait()
    made = jnp.dot(normed[n_ctx:rows, :], wq[...], preferred_element_type=F32)
    for g in range(2):
        turned = rotate(
            head_norm(made[:, g * HEAD_DIM : (g + 1) * HEAD_DIM], query_gain[...]), [(n_ctx, seq)]
        ).astype(BF16)
        for j in range(n_tp):
            q_s[pl.ds((2 * j + g) * tok, tok)] = turned[j * tok : (j + 1) * tok]
    pull(1, 2)
    for part_of in range(2):
        attend(part_of * seq, seq, kv_r[0, 0, body_rows], kv_r[0, 1, body_rows], first=True)

    def both(slot, kind):
        return jnp.concatenate([kv_r[slot, kind, body_rows], kv_l[slot, kind, body_rows]], 0)

    def step(s, carry):
        for part_of in range(2):
            if part_of == 0:
                pull(s, 0)
                pull(s - 1, 3)
            else:
                pull(s, 1)
                pull(s, 2)
            attend(part_of * seq, seq, both(s - 1, 0), both(s - 1, 1))
        return carry

    lax.fori_loop(2, last, step, 0)
    pull(last, 0)
    pull(last - 1, 3)

    def contexts(kind):
        parts = [kv_r[s, kind, 0:n_ctx] for s in range(last)]
        parts += [kv_l[s, kind, 0:n_ctx] for s in range(1, last)]
        return jnp.concatenate(parts, 0)

    for part_of in range(2):
        attend(
            part_of * seq,
            seq,
            both(last - 1, 0),
            both(last - 1, 1),
            extra=(contexts(0), contexts(1)),
        )

    cut = bounds[2][0]

    def ending(kind):
        return jnp.concatenate([kv_r[last, kind, n_ctx:cut], kv_l[last, kind, cut:rows]], 0)

    for j in range(1, n_tp):
        pull(last, j)
    for group in ((3,), (1, 2), (0,)):
        for j in group:
            att = attend(
                2 * j * tok,
                2 * tok,
                ending(0),
                ending(1),
                extra=(kv_r[last, 0, 0:n_ctx], kv_r[last, 1, 0:n_ctx]),
                final=True,
            )
            for g in range(2):
                one = att[g * tok : (g + 1) * tok]
                if j == 0:
                    att_all[x, :, pl.ds(g * HEAD_DIM, HEAD_DIM)] = one
                else:
                    att_send[j - 1, :, pl.ds(g * HEAD_DIM, HEAD_DIM)] = one
        for j in group:
            if j > 0:
                copy = remote(
                    att_send.at[j - 1],
                    att_all.at[x],
                    o_send.at[0],
                    o_recv.at[j - 1],
                    tp=tp(RELATIVE[j]),
                )
                copy.start()
    load_wo.wait()
    load_out_gain.wait()

    def channel_block(b):
        floats = att_all[b].astype(F32)
        return jnp.sum(floats * floats, -1, keepdims=True)

    square = channel_block(x)
    for j in (1, 2, 3):
        source = tp(-RELATIVE[j])
        whole = att_all.at[source]
        remote(whole, whole, o_send.at[0], o_recv.at[j - 1], tp=tp(1)).wait_recv()
        square = square + channel_block(source)

    channels = att_all.shape[2]
    inv = lax.rsqrt(square * (1.0 / (n_tp * channels)) + EPSILON)
    for b in range(n_tp):
        gain = out_gain[:, b * channels : (b + 1) * channels]
        att_n[:, b * channels : (b + 1) * channels] = (
            att_all[b].astype(F32) * inv * gain
        ).astype(BF16)
    strip = 512
    for i in range(width // strip):
        at = pl.ds(i * strip, strip)
        mix = jnp.dot(att_n[...], wo[:, at], preferred_element_type=F32)
        result[0, :, at] = (lat[0, :, at].astype(F32) + rows_mod[4:5, at] * mix).astype(BF16)

    def sent(whole, sem):
        remote(whole, whole, sem, p1_recv.at[0], sp=mate).wait_send()

    sent(lat.at[0:3], x_send.at[0])

    @pl.when(core == 0)
    def _():
        sent(other_got, p1_send.at[0])

    @pl.when(core == 1)
    def _():
        sent(own_got, p1_send.at[0])
        sent(got_half, h_send.at[0])
        sent(both_got.at[:, used], p2_send.at[0])

    sent(kv_r.at[0 : last - 1], r_send.at[0])
    sent(kv_l.at[0 : last - 1], r_send.at[1])
    at, _ = bounds[2]
    sent(kv_r.at[last - 1, :, 0:at], r_send.at[2])
    sent(kv_l.at[last - 1, :, at:rows], r_send.at[3])
    sent(att_send, o_send.at[0])


def on_device(mesh, *args):
    (
        latent,
        cond,
        context,
        cond_ctx,
        w_shift,
        w_scale,
        w_gate,
        norm_gain,
        w_query,
        w_key,
        w_value,
        query_gain,
        key_gain,
        ctx_lift,
        out_gain,
        w_out,
    ) = args
    n_sp, n_tp = mesh.shape["sp"], mesh.shape["tp"]
    assert mesh.shape["dp"] == 2
    assert n_tp == 4 and KV_HEADS == n_tp and n_sp == 16
    assert w_shift.shape == (128, 512)
    tok, width = latent.shape[1:]
    n_ctx = context.shape[1]
    rows = n_ctx + n_tp * tok
    seq = n_tp * tok
    slots = n_sp // 2 + 1
    any_ = pl.BlockSpec(memory_space=pl.ANY)
    smem = pl.BlockSpec(memory_space=pltpu.SMEM)
    dma = pltpu.SemaphoreType.DMA
    scratch = [
        pltpu.VMEM((1, width), BF16),
        pltpu.VMEM((width // 128, 128), BF16),
        pltpu.VMEM((1, width), F32),
        pltpu.VMEM((1, HEAD_DIM), F32),
        pltpu.VMEM((1, HEAD_DIM), F32),
        pltpu.VMEM((1, HEADS * HEAD_DIM), F32),
        pltpu.VMEM((n_tp, tok, width), BF16),
        pltpu.VMEM((n_ctx, width), BF16),
        pltpu.VMEM((3,) + w_shift.shape, BF16),
        pltpu.VMEM(w_query.shape, BF16),
        pltpu.VMEM((width, 2 * HEAD_DIM), BF16),
        pltpu.VMEM(w_out.shape, BF16),
        pltpu.VMEM((2, 16, 128), F32),
        pltpu.VMEM((n_sp - 1, 16, 128), F32),
        pltpu.VMEM((2, 10, 128), F32),
        pltpu.VMEM((4, 10, 128), F32),
        pltpu.VMEM((2, 10, 128), F32),
        pltpu.VMEM((n_tp, 2, 16, 128), F32),
        pltpu.VMEM((8, width), F32),
        pltpu.VMEM((rows, width), F32),
        pltpu.VMEM((rows, width), BF16),
        pltpu.VMEM((rows, HEAD_DIM), F32),
        pltpu.VMEM((rows, HEAD_DIM), F32),
        pltpu.VMEM((slots, 2, rows, HEAD_DIM), BF16),
        pltpu.VMEM((slots, 2, rows, HEAD_DIM), BF16),
        pltpu.VMEM((2 * seq, HEAD_DIM), BF16),
        pltpu.VMEM((2 * seq, 1), F32),
        pltpu.VMEM((2 * seq, 128), F32),
        pltpu.VMEM((2 * seq, 128), F32),
        pltpu.VMEM((2 * seq, HEAD_DIM), F32),
        pltpu.VMEM((n_tp - 1, tok, 2 * HEAD_DIM), BF16),
        pltpu.VMEM((n_tp, tok, 2 * HEAD_DIM), BF16),
        pltpu.VMEM((tok, HEADS * HEAD_DIM), BF16),
        dma((12,)),
        dma((1,)),
        dma((5,)),
        dma((1,)),
        dma((2,)),
        dma((1,)),
        dma((4,)),
        dma((1,)),
        dma((8,)),
        dma((4,)),
        dma((2, slots - 1, 4)),
        dma((1,)),
        dma((3,)),
    ]
    specs = [any_] * 13 + [smem, any_, any_]
    row = lambda a: a.reshape(1, -1)
    return pl.pallas_call(
        functools.partial(kernel, n_sp),
        out_shape=pltpu.VMEM(latent.shape, BF16),
        in_specs=specs,
        out_specs=pl.BlockSpec(memory_space=pltpu.VMEM),
        scratch_shapes=scratch,
        compiler_params=pltpu.CompilerParams(
            collective_id=0, has_side_effects=True, vmem_limit_bytes=56 << 20
        ),
    )(
        latent,
        cond,
        context,
        cond_ctx.reshape(-1, 128),
        w_shift,
        w_scale,
        w_gate,
        row(norm_gain),
        w_query,
        w_key,
        w_value,
        row(query_gain),
        row(key_gain),
        ctx_lift,
        row(out_gain),
        w_out,
    )


def solution(mesh):
    in_specs = (
        P(("grp", "dp"), ("sp", "tp"), None),
        P(("grp", "dp"), None),
        P(("grp", "dp"), "sp", None),
        P(),
        P("sp", "tp"),
        P("sp", "tp"),
        P("sp", "tp"),
        P(),
        P(None, "tp"),
        P(None, "tp"),
        P(None, "tp"),
        P(),
        P(),
        P("tp"),
        P(),
        P(),
    )
    out_specs = P(("grp", "dp"), ("sp", "tp"), None)
    return jax.shard_map(
        functools.partial(on_device, mesh),
        mesh=mesh,
        in_specs=in_specs,
        out_specs=out_specs,
        check_vma=False,
    )
```

```python
import functools
import math

import jax
import jax.numpy as jnp
from jax import lax
from jax.experimental import pallas as pl
from jax.experimental.pallas import tpu as pltpu
from jax.sharding import PartitionSpec as P

HEADS = 8
KV_HEADS = 4
HEAD_DIM = 128
GRID_WIDTH = 64
EPSILON = 1e-06
LOG2E = math.log2(math.e)
MESH = pl.DeviceIdType.MESH
F32 = jnp.float32
BF16 = jnp.bfloat16
RELATIVE = (0, 3, 1, 2)


def kernel(
    n_sp,
    latent,
    cond_h,
    context,
    cond_ctx_h,
    w_shift,
    w_scale,
    w_gate,
    norm_gain_h,
    w_query,
    w_key,
    w_value,
    query_gain_h,
    key_gain_h,
    ctx_lift,
    out_gain_h,
    w_out,
    result,
    cond,
    cond_ctx,
    norm_gain,
    query_gain,
    key_gain,
    out_gain,
    lat,
    ctx_rows,
    wm,
    wq,
    wkv,
    wo,
    part,
    both_got,
    window,
    got_half,
    own_mod,
    mod_all,
    rows_mod,
    unit,
    normed,
    cos_t,
    sin_t,
    kv_r,
    kv_l,
    q_s,
    lift_s,
    m_s,
    l_s,
    acc_s,
    att_send,
    att_all,
    att_n,
    loc,
    x_send,
    x_recv,
    p1_send,
    p1_recv,
    h_send,
    h_recv,
    p2_send,
    p2_recv,
    r_send,
    r_recv,
    o_send,
    o_recv,
):
    z = lax.axis_index("sp")
    x = lax.axis_index("tp")
    core = lax.axis_index("dp")
    n_tp = 4
    tok = lat.shape[1]
    half = tok // 2
    n_ctx = ctx_rows.shape[0]
    seq = n_tp * tok
    rows = n_ctx + seq
    width = lat.shape[2]
    reach = n_sp // 4
    got_mod = both_got.at[0 : n_sp // 2 - 1]
    got_other = both_got.at[n_sp // 2 - 1 : n_sp - 1]
    mate = z + 1 - 2 * lax.rem(z, 2)
    parity = lax.rem(z, 2)

    def sp(d):
        return lax.rem(z + d + n_sp, n_sp)

    def tp(d):
        return lax.rem(x + d + n_tp, n_tp)

    def remote(src, dst, s, r, **where):
        return pltpu.make_async_remote_copy(
            src_ref=src,
            dst_ref=dst,
            send_sem=s,
            recv_sem=r,
            device_id=where,
            device_id_type=MESH,
        )

    def each(start, stop, f):
        def body(i, carry):
            f(i)
            return carry

        lax.fori_loop(start, stop, body, 0)

    barrier = pltpu.get_barrier_semaphore()

    def greet(**where):
        pl.semaphore_signal(barrier, inc=1, device_id=where, device_id_type=MESH)

    @pl.when(core == 0)
    def _():
        for d in range(reach, 0, -1):
            greet(sp=sp(d), dp=1)
            greet(sp=sp(-d), dp=1)
        greet(dp=1)
        for d in (2, 1, 3):
            greet(tp=tp(d))
            greet(tp=tp(d), dp=1)
            greet(tp=tp(d), sp=mate, dp=1)
        greet(sp=sp(1))
        greet(sp=sp(-1))

    @pl.when(core == 1)
    def _():
        for d in range(reach, 0, -1):
            for to in range(2):
                greet(sp=sp(d), dp=to)
                greet(sp=sp(-d), dp=to)
        greet(dp=0)
        for d in (2, 1, 3):
            for to in (1, 0):
                greet(tp=tp(d), dp=to)
                greet(tp=tp(d), sp=mate, dp=to)

    common = 2 * reach + 2 * (n_tp - 1)
    greeted = jnp.where(core == 0, common + 2 + n_tp, 2 * common + 1)

    def load(src, dst, i):
        copy = pltpu.make_async_copy(src, dst, loc.at[i])
        copy.start()
        return copy

    load_cond = load(cond_h, cond, 0)
    load_cond_ctx = load(cond_ctx_h, cond_ctx, 1)
    for kind, matrix in enumerate((w_shift, w_scale, w_gate)):
        load(matrix, wm.at[kind], 2)
    load_lat = load(latent.at[0], lat.at[0], 3)
    load_ctx = load(context.at[0], ctx_rows, 4)
    load(w_key, wkv.at[:, pl.ds(0, HEAD_DIM)], 5)
    load(w_value, wkv.at[:, pl.ds(HEAD_DIM, HEAD_DIM)], 5)
    load_gain = load(norm_gain_h, norm_gain, 6)
    load_key_gain = load(key_gain_h, key_gain, 7)
    load_wq = load(w_query, wq, 8)
    load_query_gain = load(query_gain_h, query_gain, 9)
    load_wo = load(w_out, wo, 10)
    load_out_gain = load(out_gain_h, out_gain, 11)

    def arrived(whole, i):
        pltpu.make_async_copy(whole, whole, loc.at[i]).wait()

    in_rows = wm.shape[1]
    load_cond.wait()
    load_cond_ctx.wait()
    lanes = pl.ds(pl.multiple_of(z * in_rows, in_rows), in_rows)
    own_in = cond[:, lanes].astype(F32)
    every = cond_ctx[...].astype(F32)
    line = lax.broadcasted_iota(jnp.int32, every.shape, 0)
    ctx_in = jnp.sum(jnp.where(line == z, every, 0.0), 0, keepdims=True)
    first_row = lax.broadcasted_iota(jnp.int32, (16, in_rows), 0) == 0
    both = jnp.where(
        first_row,
        jnp.broadcast_to(own_in, (16, in_rows)),
        jnp.broadcast_to(ctx_in, (16, in_rows)),
    )
    activated = jax.nn.silu(both).astype(BF16)
    arrived(wm, 2)
    for kind in range(3):
        product = jnp.dot(activated, wm[kind], preferred_element_type=F32)
        for who in range(2 if kind < 2 else 1):
            for block in range(2):
                for side in range(2):
                    at = (2 * block + side) * 128
                    row = (2 * kind + who) * 2 + side
                    part[block, row : row + 1, :] = product[who : who + 1, at : at + 128]

    load_lat.wait()
    pl.semaphore_wait(barrier, greeted)

    used = pl.ds(0, 10)
    offsets = [o for i in range(reach, 0, -1) for o in (i, -i) if o > -reach]

    def p1(own, i, o):
        return remote(
            part.at[lax.rem(sp(-o), 2), used],
            (got_mod if own else got_other).at[i, used],
            p1_send.at[0],
            p1_recv.at[0 if own else 1],
            sp=sp(-o),
            dp=1,
        )

    @pl.when(core == 1)
    def _():
        for i, o in enumerate(offsets):
            p1(True, i, o).start()

    @pl.when(core == 0)
    def _():
        for i, o in enumerate(offsets + [0]):
            p1(False, i, o).start()

    lo, hi = pl.ds(0, half), pl.ds(half, half)
    x_copies = [
        remote(lat.at[0, lo], lat.at[1, lo], x_send.at[0], x_recv.at[0], tp=tp(1)),
        remote(lat.at[0, hi], lat.at[2, hi], x_send.at[0], x_recv.at[1], tp=tp(-1)),
        remote(lat.at[0, hi], lat.at[1, hi], x_send.at[0], x_recv.at[2], tp=tp(1)),
        remote(lat.at[0, lo], lat.at[2, lo], x_send.at[0], x_recv.at[3], tp=tp(-1)),
        remote(lat.at[1, lo], lat.at[3, lo], x_send.at[0], x_recv.at[4], tp=tp(1)),
        remote(lat.at[2, hi], lat.at[3, hi], x_send.at[0], x_recv.at[4], tp=tp(-1)),
    ]
    for copy in x_copies[:4]:
        copy.start()

    cos_t[0:n_ctx, :] = jnp.ones((n_ctx, HEAD_DIM), F32)
    sin_t[0:n_ctx, :] = jnp.zeros((n_ctx, HEAD_DIM), F32)
    lane = lax.broadcasted_iota(jnp.int32, (tok, HEAD_DIM), 1)
    place = lax.broadcasted_iota(jnp.int32, (tok, HEAD_DIM), 0)
    quarter = HEAD_DIM // 4
    inverse = jnp.exp((lane & (quarter - 1)).astype(F32) * (-math.log(10000.0) / quarter))
    lower = (lane & (2 * quarter - 1)) < quarter
    for j in range(n_tp):
        token = z * seq + tp(RELATIVE[j]) * tok + place
        grid_row = token >> (GRID_WIDTH.bit_length() - 1)
        grid_col = token & (GRID_WIDTH - 1)
        angle = jnp.where(lane < 2 * quarter, grid_row, grid_col).astype(F32) * inverse
        at = n_ctx + j * tok
        cos_t[at : at + tok, :] = jnp.cos(angle)
        sine = jnp.sin(angle)
        sin_t[at : at + tok, :] = jnp.where(lower, -sine, sine)

    for g in range(2):
        lift = (ctx_lift[g] + math.log(seq / n_ctx)) * LOG2E
        for j in range(n_tp):
            lift_s[pl.ds((2 * j + g) * tok, tok)] = jnp.full((tok, 1), lift, F32)

    def prepare(read, base, count):
        def body(i, carry):
            floats = read(pl.ds(pl.multiple_of(i * 16, 16), 16)).astype(F32)
            inv = lax.rsqrt(jnp.mean(floats * floats, -1, keepdims=True) + EPSILON)
            unit[pl.ds(pl.multiple_of(base + i * 16, 16), 16), :] = floats * inv
            return carry

        lax.fori_loop(0, count // 16, body, 0)

    load_ctx.wait()
    prepare(lambda i: ctx_rows[i, :], 0, n_ctx)
    prepare(lambda i: lat[0, i, :], n_ctx, tok)
    arrived(wkv, 5)
    load_gain.wait()
    load_key_gain.wait()

    own_got = got_mod.at[:, used]
    other_got = got_other.at[:, used]

    def half_window(own, i):
        return remote(
            window.at[0 if own else 1],
            got_half.at[i if own else 2 + i],
            h_send.at[0],
            h_recv.at[i if own else 2 + i],
            sp=sp((reach, -reach)[i]),
        )

    spread = [(d, e) for e in (1, 0) for d in (2, 1, 3, 0)]

    def p2(core_of, i):
        d, e = spread[i]
        where = dict(dp=core_of)
        if d:
            where["tp"] = tp(d)
        if e:
            where["sp"] = mate
        return remote(
            own_mod.at[1 - core_of],
            mod_all.at[x, parity, used],
            p2_send.at[0],
            p2_recv.at[0],
            **where,
        )

    @pl.when(core == 1)
    def _():
        remote(own_got, own_got, p1_send.at[0], p1_recv.at[0], sp=mate).wait_recv()
        window[0] = sum((got_mod[i, 0:10, :] for i in range(len(offsets))), part[parity, 0:10, :])
        for i in range(2):
            half_window(True, i).start()
        remote(other_got, other_got, p1_send.at[0], p1_recv.at[1], sp=mate).wait_recv()
        window[1] = sum(got_other[i, 0:10, :] for i in range(len(offsets) + 1))
        for i in range(2):
            half_window(False, i).start()
        for i in range(2):
            half_window(True, i).wait_recv()
        own_mod[0] = got_half[0] + got_half[1]
        mod_all[x, parity, 0:10, :] = own_mod[0]
        for i in range(7):
            p2(1, i).start()
        for i in range(2):
            half_window(False, i).wait_recv()
        own_mod[1] = got_half[2] + got_half[3]
        for i in range(8):
            p2(0, i).start()

    x_copies[0].wait_recv()
    x_copies[4].start()
    x_copies[1].wait_recv()
    x_copies[5].start()
    prepare(lambda i: lat[1, i, :], n_ctx + tok, half)
    prepare(lambda i: lat[2, pl.ds(half + i.start, i.size), :], n_ctx + 2 * tok + half, half)
    for count in (7, 8):

        @pl.when(core == 8 - count)
        def _(count=count):
            tiles = both_got.at[0:count, used]
            remote(tiles, tiles, p2_send.at[0], p2_recv.at[0], sp=mate).wait_recv()


    cols = width // n_tp
    for b in range(n_tp):
        for block in range(2):
            tile = mod_all[b, block, 0:10, :]
            for side in range(2):
                at = b * cols + (2 * block + side) * 128
                gain = norm_gain[:, at : at + 128]
                for who in range(2):
                    r = who * 2 + side
                    rows_mod[who : who + 1, at : at + 128] = tile[r : r + 1, :]
                    rows_mod[2 + who : 3 + who, at : at + 128] = gain * (
                        1.0 + tile[4 + r : 5 + r, :]
                    )
                rows_mod[4:5, at : at + 128] = tile[8 + side : 9 + side, :]

    def norm_rows(base, count, who):
        shift = rows_mod[who : who + 1, :]
        scale = rows_mod[2 + who : 3 + who, :]

        def body(i, carry):
            at = pl.ds(pl.multiple_of(base + i * 16, 16), 16)
            normed[at, :] = (unit[at, :] * scale + shift).astype(BF16)
            return carry

        lax.fori_loop(0, count // 16, body, 0)

    def head_norm(raw, gain):
        floats = raw.astype(BF16).astype(F32)
        return floats * lax.rsqrt(jnp.mean(floats * floats, -1, keepdims=True) + EPSILON) * gain

    def rotate(vectors, pieces):
        d = lax.broadcasted_iota(jnp.int32, vectors.shape, 1)
        cosine = jnp.concatenate([cos_t[b : b + n, :] for b, n in pieces], 0)
        sine = jnp.concatenate([sin_t[b : b + n, :] for b, n in pieces], 0)
        swapped = jnp.where(
            (d & (2 * quarter - 1)) < quarter,
            pltpu.roll(vectors, HEAD_DIM - quarter, 1),
            pltpu.roll(vectors, quarter, 1),
        )
        return vectors * cosine + swapped * sine

    second, third = n_ctx + tok, n_ctx + 2 * tok
    chunk_rows = [
        [(0, n_ctx + tok)],
        [(second, half), (third + half, half)],
        [(second + half, half), (third, half)],
        [(n_ctx + 3 * tok, tok)],
    ]

    bounds = [(0, n_ctx + tok)] + [(n_ctx + j * tok, tok) for j in range(1, n_tp)]

    def ring(way, slot, j, final=False):
        at, count = bounds[j]
        buf = kv_r if way == 0 else kv_l
        piece = pl.ds(at, count)
        target = sp(1) if way == 0 else sp(-1)
        return remote(
            buf.at[slot - 1, :, piece],
            buf.at[slot, :, piece],
            r_send.at[way + 2 if final else way],
            r_recv.at[slot - 1, j],
            sp=target,
        )

    last = n_sp // 2
    factor = LOG2E * HEAD_DIM ** (-0.5)
    nt = (((1,), (1,)), ((), ()))

    def attend(at, count, keys, values, extra=None, first=False, final=False):
        here = pl.ds(at, count)
        queries = q_s[here]
        scores = lax.dot_general(queries, keys, nt, preferred_element_type=F32) * factor
        if extra is not None:
            more = lax.dot_general(queries, extra[0], nt, preferred_element_type=F32) * factor
            scores = jnp.concatenate([scores, more + lift_s[here]], 1)
            values = jnp.concatenate([values, extra[1]], 0)
        top = jnp.broadcast_to(jnp.max(scores, -1, keepdims=True), (count, 128))
        if not first:
            before = m_s[here]
            top = jnp.maximum(before, top)
        size = scores.shape[1]
        wide = jnp.concatenate([top] * (size // 128) + [top[:, : size % 128]] * (size % 128 > 0), 1)
        weights = jnp.exp2(scores - wide)
        full = weights.shape[1] // 128 * 128
        total = sum(weights[:, i : i + 128] for i in range(0, full, 128))
        if full < weights.shape[1]:
            rest = jnp.sum(weights[:, full:], -1, keepdims=True)
            one = lax.broadcasted_iota(jnp.int32, total.shape, 1) == 0
            total = total + jnp.where(one, rest, 0.0)
        out = jnp.dot(weights.astype(BF16), values, preferred_element_type=F32)
        if not first:
            keep = jnp.exp2(before - top)
            total = total + l_s[here] * keep
            out = out + acc_s[here] * keep
        if final:
            return (out / jnp.sum(total, -1, keepdims=True)).astype(BF16)
        m_s[here] = top
        l_s[here] = total
        acc_s[here] = out

    def pull(s, j):
        at, count = bounds[j]
        own_way = 0 if j < 2 else 1

        def final():
            ring(own_way, last, j, True).start()

        if isinstance(s, int) and s == last:
            ring(own_way, s, j).wait_recv()
            return
        pair = kv_r.at[0:2, :, pl.ds(at, count)]
        remote(pair, pair, r_send.at[0], r_recv.at[s - 1, j], sp=mate).wait_recv()

        def forward():
            for way in range(2):
                ring(way, s + 1, j).start()

        if isinstance(s, int):
            (forward if s + 1 < last else final)()
        else:
            pl.when(s + 1 < last)(forward)
            pl.when(s + 1 == last)(final)

    norm_rows(0, n_ctx, 1)
    norm_rows(n_ctx, tok, 0)

    def produce(j):
        at, count = bounds[j]
        if j == 2:
            x_copies[2].wait_recv()
            x_copies[3].wait_recv()
            prepare(lambda i: lat[1, pl.ds(half + i.start, i.size), :], second + half, half)
            prepare(lambda i: lat[2, i, :], third, half)
        if j == 3:
            remote(lat.at[3], lat.at[3], x_send.at[0], x_recv.at[4], tp=tp(1)).wait_recv()
            prepare(lambda i: lat[3, i, :], n_ctx + 3 * tok, tok)
        pieces = chunk_rows[j]
        if j > 0:
            for begin, size in pieces:
                norm_rows(begin, size, 0)
        inputs = jnp.concatenate([normed[b : b + n, :] for b, n in pieces], 0)
        made = jnp.dot(inputs, wkv[...], preferred_element_type=F32)
        keys = rotate(head_norm(made[:, :HEAD_DIM], key_gain[...]), pieces).astype(BF16)
        values = made[:, HEAD_DIM:].astype(BF16)
        kv_r[0, 0, at : at + count, :] = keys
        kv_l[0, 0, at : at + count, :] = keys
        kv_r[0, 1, at : at + count, :] = values
        kv_l[0, 1, at : at + count, :] = values
        ring(0, 1, j).start()
        ring(1, 1, j).start()

    body_rows = pl.ds(n_ctx, seq)
    produce(0)
    produce(1)
    produce(2)
    pull(1, 0)
    produce(3)
    pull(1, 1)
    load_wq.wait()
    load_query_gain.wait()
    made = jnp.dot(normed[n_ctx:rows, :], wq[...], preferred_element_type=F32)
    for g in range(2):
        turned = rotate(
            head_norm(made[:, g * HEAD_DIM : (g + 1) * HEAD_DIM], query_gain[...]), [(n_ctx, seq)]
        ).astype(BF16)
        for j in range(n_tp):
            q_s[pl.ds((2 * j + g) * tok, tok)] = turned[j * tok : (j + 1) * tok]
    pull(1, 2)
    for part_of in range(2):
        attend(part_of * seq, seq, kv_r[0, 0, body_rows], kv_r[0, 1, body_rows], first=True)

    def both(slot, kind):
        return jnp.concatenate([kv_r[slot, kind, body_rows], kv_l[slot, kind, body_rows]], 0)

    def step(s, carry):
        for part_of in range(2):
            if part_of == 0:
                pull(s, 0)
                pull(s - 1, 3)
            else:
                pull(s, 1)
                pull(s, 2)
            attend(part_of * seq, seq, both(s - 1, 0), both(s - 1, 1))
        return carry

    lax.fori_loop(2, last, step, 0)
    pull(last, 0)
    pull(last - 1, 3)

    def contexts(kind):
        parts = [kv_r[s, kind, 0:n_ctx] for s in range(last)]
        parts += [kv_l[s, kind, 0:n_ctx] for s in range(1, last)]
        return jnp.concatenate(parts, 0)

    for part_of in range(2):
        attend(
            part_of * seq,
            seq,
            both(last - 1, 0),
            both(last - 1, 1),
            extra=(contexts(0), contexts(1)),
        )

    cut = bounds[2][0]

    def ending(kind):
        return jnp.concatenate([kv_r[last, kind, n_ctx:cut], kv_l[last, kind, cut:rows]], 0)

    for j in range(1, n_tp):
        pull(last, j)
    for group in ((3,), (1, 2), (0,)):
        for j in group:
            att = attend(
                2 * j * tok,
                2 * tok,
                ending(0),
                ending(1),
                extra=(kv_r[last, 0, 0:n_ctx], kv_r[last, 1, 0:n_ctx]),
                final=True,
            )
            for g in range(2):
                one = att[g * tok : (g + 1) * tok]
                if j == 0:
                    att_all[x, :, pl.ds(g * HEAD_DIM, HEAD_DIM)] = one
                else:
                    att_send[j - 1, :, pl.ds(g * HEAD_DIM, HEAD_DIM)] = one
        for j in group:
            if j > 0:
                copy = remote(
                    att_send.at[j - 1],
                    att_all.at[x],
                    o_send.at[0],
                    o_recv.at[j - 1],
                    tp=tp(RELATIVE[j]),
                )
                copy.start()
    load_wo.wait()
    load_out_gain.wait()

    def channel_block(b):
        floats = att_all[b].astype(F32)
        return jnp.sum(floats * floats, -1, keepdims=True)

    square = channel_block(x)
    for j in (1, 2, 3):
        source = tp(-RELATIVE[j])
        whole = att_all.at[source]
        remote(whole, whole, o_send.at[0], o_recv.at[j - 1], tp=tp(1)).wait_recv()
        square = square + channel_block(source)

    channels = att_all.shape[2]
    inv = lax.rsqrt(square * (1.0 / (n_tp * channels)) + EPSILON)
    for b in range(n_tp):
        gain = out_gain[:, b * channels : (b + 1) * channels]
        att_n[:, b * channels : (b + 1) * channels] = (
            att_all[b].astype(F32) * inv * gain
        ).astype(BF16)
    strip = 512
    for i in range(width // strip):
        at = pl.ds(i * strip, strip)
        mix = jnp.dot(att_n[...], wo[:, at], preferred_element_type=F32)
        result[0, :, at] = (lat[0, :, at].astype(F32) + rows_mod[4:5, at] * mix).astype(BF16)

    def sent(whole, sem):
        remote(whole, whole, sem, p1_recv.at[0], sp=mate).wait_send()

    sent(lat.at[0:3], x_send.at[0])

    @pl.when(core == 0)
    def _():
        sent(other_got, p1_send.at[0])

    @pl.when(core == 1)
    def _():
        sent(own_got, p1_send.at[0])
        sent(got_half, h_send.at[0])
        sent(both_got.at[:, used], p2_send.at[0])

    sent(kv_r.at[0 : last - 1], r_send.at[0])
    sent(kv_l.at[0 : last - 1], r_send.at[1])
    at, _ = bounds[2]
    sent(kv_r.at[last - 1, :, 0:at], r_send.at[2])
    sent(kv_l.at[last - 1, :, at:rows], r_send.at[3])
    sent(att_send, o_send.at[0])


def on_device(mesh, *args):
    (
        latent,
        cond,
        context,
        cond_ctx,
        w_shift,
        w_scale,
        w_gate,
        norm_gain,
        w_query,
        w_key,
        w_value,
        query_gain,
        key_gain,
        ctx_lift,
        out_gain,
        w_out,
    ) = args
    n_sp, n_tp = mesh.shape["sp"], mesh.shape["tp"]
    assert mesh.shape["dp"] == 2
    assert n_tp == 4 and KV_HEADS == n_tp and n_sp == 16
    assert w_shift.shape == (128, 512)
    tok, width = latent.shape[1:]
    n_ctx = context.shape[1]
    rows = n_ctx + n_tp * tok
    seq = n_tp * tok
    slots = n_sp // 2 + 1
    any_ = pl.BlockSpec(memory_space=pl.ANY)
    smem = pl.BlockSpec(memory_space=pltpu.SMEM)
    dma = pltpu.SemaphoreType.DMA
    scratch = [
        pltpu.VMEM((1, width), BF16),
        pltpu.VMEM((width // 128, 128), BF16),
        pltpu.VMEM((1, width), F32),
        pltpu.VMEM((1, HEAD_DIM), F32),
        pltpu.VMEM((1, HEAD_DIM), F32),
        pltpu.VMEM((1, HEADS * HEAD_DIM), F32),
        pltpu.VMEM((n_tp, tok, width), BF16),
        pltpu.VMEM((n_ctx, width), BF16),
        pltpu.VMEM((3,) + w_shift.shape, BF16),
        pltpu.VMEM(w_query.shape, BF16),
        pltpu.VMEM((width, 2 * HEAD_DIM), BF16),
        pltpu.VMEM(w_out.shape, BF16),
        pltpu.VMEM((2, 16, 128), F32),
        pltpu.VMEM((n_sp - 1, 16, 128), F32),
        pltpu.VMEM((2, 10, 128), F32),
        pltpu.VMEM((4, 10, 128), F32),
        pltpu.VMEM((2, 10, 128), F32),
        pltpu.VMEM((n_tp, 2, 16, 128), F32),
        pltpu.VMEM((8, width), F32),
        pltpu.VMEM((rows, width), F32),
        pltpu.VMEM((rows, width), BF16),
        pltpu.VMEM((rows, HEAD_DIM), F32),
        pltpu.VMEM((rows, HEAD_DIM), F32),
        pltpu.VMEM((slots, 2, rows, HEAD_DIM), BF16),
        pltpu.VMEM((slots, 2, rows, HEAD_DIM), BF16),
        pltpu.VMEM((2 * seq, HEAD_DIM), BF16),
        pltpu.VMEM((2 * seq, 1), F32),
        pltpu.VMEM((2 * seq, 128), F32),
        pltpu.VMEM((2 * seq, 128), F32),
        pltpu.VMEM((2 * seq, HEAD_DIM), F32),
        pltpu.VMEM((n_tp - 1, tok, 2 * HEAD_DIM), BF16),
        pltpu.VMEM((n_tp, tok, 2 * HEAD_DIM), BF16),
        pltpu.VMEM((tok, HEADS * HEAD_DIM), BF16),
        dma((12,)),
        dma((1,)),
        dma((5,)),
        dma((1,)),
        dma((2,)),
        dma((1,)),
        dma((4,)),
        dma((1,)),
        dma((1,)),
        dma((4,)),
        dma((slots - 1, 4)),
        dma((1,)),
        dma((3,)),
    ]
    specs = [any_] * 13 + [smem, any_, any_]
    row = lambda a: a.reshape(1, -1)
    return pl.pallas_call(
        functools.partial(kernel, n_sp),
        out_shape=pltpu.VMEM(latent.shape, BF16),
        in_specs=specs,
        out_specs=pl.BlockSpec(memory_space=pltpu.VMEM),
        scratch_shapes=scratch,
        compiler_params=pltpu.CompilerParams(
            collective_id=0, has_side_effects=True, vmem_limit_bytes=56 << 20
        ),
    )(
        latent,
        cond,
        context,
        cond_ctx.reshape(-1, 128),
        w_shift,
        w_scale,
        w_gate,
        row(norm_gain),
        w_query,
        w_key,
        w_value,
        row(query_gain),
        row(key_gain),
        ctx_lift,
        row(out_gain),
        w_out,
    )


def solution(mesh):
    in_specs = (
        P(("grp", "dp"), ("sp", "tp"), None),
        P(("grp", "dp"), None),
        P(("grp", "dp"), "sp", None),
        P(),
        P("sp", "tp"),
        P("sp", "tp"),
        P("sp", "tp"),
        P(),
        P(None, "tp"),
        P(None, "tp"),
        P(None, "tp"),
        P(),
        P(),
        P("tp"),
        P(),
        P(),
    )
    out_specs = P(("grp", "dp"), ("sp", "tp"), None)
    return jax.shard_map(
        functools.partial(on_device, mesh),
        mesh=mesh,
        in_specs=in_specs,
        out_specs=out_specs,
        check_vma=False,
    )
```
